256 devices in a mesh: rep: 32 (over z, y), fs: 4 (over x), tp: 2 (over core).
Axes of the slice: x: 4, y: 4, z: 8, core: 2. Of those that a mesh axis runs over, the one named last changes fastest.
Arguments:
- tokens: bfloat16 [32768, 2048], P(('rep', 'fs', 'tp')), may hold values from -24 to 24
- cotangent: bfloat16 [32768, 2048], P(('rep', 'fs', 'tp')), may hold values from -24 to 24
- gate_weight: bfloat16 [2048, 3072], P(None, 'fs'), may hold values from -0.125 to 0.125
- up_weight: bfloat16 [2048, 3072], P(None, 'fs'), may hold values from -0.125 to 0.125
- down_weight_t: bfloat16 [2048, 3072], P(None, 'fs'), may hold values from -0.109375 to 0.109375
Outputs:
- input_grad: bfloat16 [32768, 2048], P(('rep', 'fs', 'tp'))
- gate_grad: float32 [2048, 3072], P(('rep', 'tp'), 'fs')
- up_grad: float32 [2048, 3072], P(('rep', 'tp'), 'fs')
- down_grad: float32 [2048, 3072], P(('rep', 'tp'), 'fs')
The draws below stay inside these ranges and needn't reach their ends.
All inputs are finite; a program needn't handle non-finite values.
Results may differ from the reference program's by a relative error of at most 0.012.
Values may be sent and summed in bfloat16 or wider, within the bound.
No kernel may reach another device: no remote copies, remote signals or barrier semaphores. Data moves between devices by JAX's collectives and lax.ppermute only.
A program may use at most 128 MiB of HBM per device.

```python
import jax
import jax.numpy as jnp
from jax import lax

D = 2048
FF = 3072
TOKENS = 32768
N_REP = 32
N_FS = 4


def raised(result, rng, source, target, blocks, factor):
    def block_of(axis_at):
        return (jnp.arange(result.shape[axis_at]) // (result.shape[axis_at] // blocks)).reshape((-1,) + (1,) * (result.ndim - 1 - axis_at))

    first = jax.random.permutation(rng, blocks)[block_of(target)]
    other_side = (block_of(target) + blocks // 2) % blocks
    return jnp.where((block_of(source) == first) | (block_of(source) == other_side), factor * result, result)


def block_levels(rng, shape, shards, low, top_value):
    def one(dim, shards_of):
        heights = jax.random.uniform(jax.random.fold_in(jax.random.fold_in(rng, 6), dim), (shards_of,), jnp.float32, low / len(shards), top_value / len(shards))
        return jnp.repeat(jnp.exp(heights), shape[dim] // shards_of).reshape((-1,) + (1,) * (len(shape) - dim - 1))

    loudness = one(*shards[0])
    for cut in shards[1:]:
        loudness = loudness * one(*cut)
    return loudness


def gaussian(key, extent, width, limit, split=(), kind=jnp.bfloat16):
    loudness = block_levels(key, extent, split, -0.22, 0.18) if split else 1.0
    result = jax.random.normal(key, extent, jnp.float32) * width * loudness
    return jnp.minimum(jnp.maximum(result, -limit), limit).astype(kind)


def noise_with(key, dims, width, most, pieces, heavy, held_as=jnp.bfloat16):
    values = width * jax.random.normal(key, dims, jnp.float32)
    if pieces:
        values = values * block_levels(key, dims, pieces, -0.22, 0.18)
    return jnp.clip(raised(values, jax.random.fold_in(key, 3), *heavy), -most, most).astype(held_as)


def setup_inputs(seed: int = 0) -> dict:
    arg_keys = jax.random.split(jax.random.key(seed), 6)
    tokens = noise_with(arg_keys[0], (TOKENS, D), 1.0, 24.0, ((0, 256),), (0, 1, 256, 6.0))
    cotangent = noise_with(arg_keys[1], (TOKENS, D), 1.0, 24.0, ((0, 256),), (0, 1, 256, 6.0))
    gate_weight = gaussian(arg_keys[2], (D, FF), D ** -0.5, 0.125, ((1, 4),))
    up_weight = gaussian(arg_keys[3], (D, FF), D ** -0.5, 0.125, ((1, 4),))
    down_weight_t = gaussian(arg_keys[4], (D, FF), FF ** -0.5, 0.109375, ((1, 4),))
    return dict(tokens=tokens, cotangent=cotangent, gate_weight=gate_weight, up_weight=up_weight, down_weight_t=down_weight_t)


def reference(tokens, cotangent, gate_weight, up_weight, down_weight_t):
    row_block = TOKENS // N_REP
    hid_width = FF // N_FS
    gate_split = gate_weight.astype(jnp.float32).reshape(D, N_FS, hid_width)
    up_split = up_weight.astype(jnp.float32).reshape(D, N_FS, hid_width)

    def accumulate(totals, block_index):
        first_row = block_index * row_block
        tok_rows = lax.dynamic_slice_in_dim(tokens, first_row, row_block, 0)
        cot_rows = lax.dynamic_slice_in_dim(cotangent, first_row, row_block, 0)
        gate_pre = jnp.dot(tok_rows, gate_weight, preferred_element_type=jnp.float32)
        up_pre = jnp.dot(tok_rows, up_weight, preferred_element_type=jnp.float32)
        sig_gate = jax.nn.sigmoid(gate_pre)
        act_gate = gate_pre * sig_gate
        hidden = (act_gate * up_pre).astype(jnp.bfloat16)
        hid_grad = jnp.dot(cot_rows, down_weight_t, preferred_element_type=jnp.float32)
        gate_back = (hid_grad * up_pre * sig_gate * (1.0 + gate_pre * (1.0 - sig_gate))).astype(jnp.bfloat16)
        up_back = (hid_grad * act_gate).astype(jnp.bfloat16)
        partial_value = jnp.einsum("rnf,dnf->nrd", gate_back.astype(jnp.float32).reshape(row_block, N_FS, hid_width),
                             gate_split, precision=lax.Precision.HIGHEST)
        partial_value = partial_value + jnp.einsum("rnf,dnf->nrd", up_back.astype(jnp.float32).reshape(row_block, N_FS, hid_width),
                                       up_split, precision=lax.Precision.HIGHEST)
        rounded = lax.optimization_barrier(partial_value.astype(jnp.bfloat16))
        input_rows = jnp.sum(rounded.astype(jnp.float32), axis=0).astype(jnp.bfloat16)
        new_totals = (totals[0] + jnp.dot(tok_rows.T, gate_back, preferred_element_type=jnp.float32),
                      totals[1] + jnp.dot(tok_rows.T, up_back, preferred_element_type=jnp.float32),
                      totals[2] + jnp.dot(cot_rows.T, hidden, preferred_element_type=jnp.float32))
        return new_totals, input_rows

    zeros = jnp.zeros((D, FF), jnp.float32)
    totals, input_blocks = lax.scan(accumulate, (zeros, zeros, zeros), jnp.arange(N_REP, dtype=jnp.int32))
    grad_scale = float(TOKENS) ** -0.5
    return (input_blocks.reshape(TOKENS, D), totals[0] * grad_scale, totals[1] * grad_scale, totals[2] * grad_scale)
```

```python
import jax
import jax.numpy as jnp
from jax import lax
from jax.experimental import pallas as pl
from jax.experimental.pallas import tpu as pltpu
from jax.sharding import Mesh
from jax.sharding import PartitionSpec as P


F32 = jnp.float32
BF16 = jnp.bfloat16


def shifted(value, axis, by):
    n = lax.axis_size(axis)
    return lax.ppermute(value, axis, [(i, (i + by) % n) for i in range(n)])


def after(value, *others):
    return lax.optimization_barrier((value, *others))[0]


def ring_gather(value, first_after=()):
    half = value.shape[0] // 2
    start = after(value, *first_after) if first_after else value
    left = shifted(start, "fs", 1)
    right = shifted(start, "fs", -1)
    far_top = shifted(left[:half], "fs", 1)
    far_bottom = shifted(right[half:], "fs", -1)
    return jnp.concatenate([value, left, right, far_top, far_bottom], axis=0), (left, right)


def weight_grad(lhs, rhs):
    tokens, width = lhs.shape
    n = rhs.shape[1]
    nz, ny = lax.axis_size("z"), lax.axis_size("y")
    rows = width // (nz * ny * 2)
    block = width // nz
    place = jnp.stack([lax.axis_index("y"), lax.axis_index("tp")]).astype(jnp.int32)

    def kernel(place_ref, lhs_ref, rhs_ref, mine_ref, theirs_ref, scratch):
        y, c = place_ref[0], place_ref[1]
        out = lax.dot_general(
            lhs_ref[...], rhs_ref[...], (((0,), (0,)), ((), ())), preferred_element_type=F32
        )
        scratch[...] = out.reshape(2 * ny, rows, n)
        for rel in range(ny):
            at = 2 * ((y + rel) % ny)
            mine_ref[rel, 0] = scratch[at + c].astype(BF16)
            theirs_ref[rel, 0] = scratch[at + 1 - c].astype(BF16)

    out_spec = pl.BlockSpec((ny, 1, rows, n), lambda i, place: (0, i, 0, 0))
    shape = jax.ShapeDtypeStruct((ny, nz, rows, n), BF16)
    return pl.pallas_call(
        kernel,
        grid_spec=pltpu.PrefetchScalarGridSpec(
            num_scalar_prefetch=1,
            grid=(nz,),
            in_specs=[
                pl.BlockSpec((tokens, block), lambda i, place: (0, i)),
                pl.BlockSpec((tokens, n), lambda i, place: (0, 0)),
            ],
            out_specs=[out_spec, out_spec],
            scratch_shapes=[pltpu.VMEM((2 * ny, rows, n), F32)],
        ),
        out_shape=[shape, shape],
        cost_estimate=pl.CostEstimate(
            flops=2 * tokens * width * n, bytes_accessed=2 * (tokens * (width + n) + width * n), transcendentals=0
        ),
    )(place, lhs, rhs)


def sum_over_replicas(mine, theirs, scale):
    partner = lax.ppermute(theirs, "tp", [(0, 1), (1, 0)])
    own = mine.astype(F32) + partner.astype(F32)
    half = own.shape[1] // 2
    up_far = shifted(own[2, :half].astype(BF16), "y", 1)
    down_far = shifted(own[2, half:].astype(BF16), "y", -1)
    to_next = jnp.concatenate([own[1, :half] + up_far.astype(F32), own[1, half:]], axis=0)
    to_last = jnp.concatenate([own[3, :half], own[3, half:] + down_far.astype(F32)], axis=0)
    from_last = shifted(to_next.astype(BF16), "y", 1)
    from_next = shifted(to_last.astype(BF16), "y", -1)
    plane = (own[0] + from_last.astype(F32) + from_next.astype(F32)).astype(BF16)
    arrived = lax.all_to_all(plane, "z", split_axis=0, concat_axis=0, tiled=True)
    return arrived.astype(F32).sum(axis=0) * scale


def sum_at_owner(parts, rows):
    own, last, nxt, far = (parts[i * rows : (i + 1) * rows] for i in range(4))
    half = rows // 2
    far = far.astype(BF16)
    from_last = shifted(far[:half], "fs", 1)
    from_next = shifted(far[half:], "fs", -1)
    to_next = jnp.concatenate([nxt[:half] + from_last.astype(F32), nxt[half:]], axis=0)
    to_last = jnp.concatenate([last[:half], last[half:] + from_next.astype(F32)], axis=0)
    a = shifted(to_next.astype(BF16), "fs", 1)
    b = shifted(to_last.astype(BF16), "fs", -1)
    return (own + a.astype(F32) + b.astype(F32)).astype(BF16)


def on_device(tokens, cotangent, gate_weight, up_weight, down_weight_t):
    rows = tokens.shape[0]
    tok, first = ring_gather(tokens)
    cot, _ = ring_gather(cotangent, first)
    gate_pre = jnp.dot(tok, gate_weight, preferred_element_type=F32)
    up_pre = jnp.dot(tok, up_weight, preferred_element_type=F32)
    sig = jax.nn.sigmoid(gate_pre)
    act = gate_pre * sig
    hidden = (act * up_pre).astype(BF16)
    hid_grad = jnp.dot(cot, down_weight_t, preferred_element_type=F32)
    gate_back = (hid_grad * up_pre * sig * (1.0 + gate_pre * (1.0 - sig))).astype(BF16)
    up_back = (hid_grad * act).astype(BF16)

    n_dev = lax.axis_size("z") * lax.axis_size("y") * lax.axis_size("fs") * lax.axis_size("tp")
    scale = float(rows * n_dev) ** -0.5
    n = gate_back.shape[1]
    down_grad = sum_over_replicas(*weight_grad(cot, hidden), scale)
    both = sum_over_replicas(*weight_grad(tok, jnp.concatenate([gate_back, up_back], axis=1)), scale)

    across = (((1,), (1,)), ((), ()))
    parts = lax.dot_general(gate_back, gate_weight, across, preferred_element_type=F32) + lax.dot_general(
        up_back, up_weight, across, preferred_element_type=F32
    )
    input_grad = sum_at_owner(parts, rows)
    return input_grad, both[:, :n], both[:, n:], down_grad


def solution(mesh):
    n_rep, n_fs, n_tp = (mesh.shape[a] for a in ("rep", "fs", "tp"))
    ny = 4
    grid = Mesh(mesh.devices.reshape(n_rep // ny, ny, n_fs, n_tp), ("z", "y", "fs", "tp"))
    split = P(("z", "y", "fs", "tp"), None)
    weight = P(None, "fs")
    grad = P(("z", "y", "tp"), "fs")
    return jax.shard_map(
        on_device,
        mesh=grid,
        in_specs=(split, split, weight, weight, weight),
        out_specs=(split, grad, grad, grad),
        check_vma=False,
    )
```

```python
import jax
import jax.numpy as jnp
from jax import lax
from jax.experimental import pallas as pl
from jax.experimental.pallas import tpu as pltpu
from jax.sharding import Mesh
from jax.sharding import PartitionSpec as P


F32 = jnp.float32
BF16 = jnp.bfloat16
NT = (((1,), (1,)), ((), ()))


def shifted(value, axis, by):
    n = lax.axis_size(axis)
    return lax.ppermute(value, axis, [(i, (i + by) % n) for i in range(n)])


def total(*values):
    return sum(v.astype(F32) for v in values)


def halves(a, b):
    return jnp.concatenate([a, b], axis=0)


def ring_gather(value):
    half = value.shape[0] // 2
    left = shifted(value, "fs", 1)
    right = shifted(value, "fs", -1)
    far_top = shifted(left[:half], "fs", 1)
    far_bottom = shifted(right[half:], "fs", -1)
    return value, left, right, far_top, far_bottom


def whole(shape):
    return pl.BlockSpec(shape, lambda *_: (0,) * len(shape))


def cost(flops, *arrays):
    return pl.CostEstimate(flops=flops, bytes_accessed=sum(2 * a for a in arrays), transcendentals=0)


def turned(pieces):
    width = pieces[0].shape[1]
    rows = sum(p.shape[0] for p in pieces)
    block = 512

    def kernel(*refs):
        refs[-1][...] = jnp.concatenate([r[...] for r in refs[:-1]], axis=0).T

    return pl.pallas_call(
        kernel,
        grid=(width // block,),
        in_specs=[pl.BlockSpec((p.shape[0], block), lambda i: (0, i)) for p in pieces],
        out_specs=pl.BlockSpec((block, rows), lambda i: (i, 0)),
        out_shape=jax.ShapeDtypeStruct((width, rows), pieces[0].dtype),
        cost_estimate=cost(rows * width * 16, 2 * rows * width),
    )(*pieces)


def forward(pieces, gate_weight, up_weight):
    width, n = gate_weight.shape
    rows = sum(p.shape[0] for p in pieces)
    block = 256

    def kernel(a, b, c, d, e, gw, uw, hidden_ref, act_ref, slope_ref):
        tok = jnp.concatenate([r[...] for r in (a, b, c, d, e)], axis=0)
        gate_pre = jnp.dot(tok, gw[...], preferred_element_type=F32)
        up_pre = jnp.dot(tok, uw[...], preferred_element_type=F32)
        sig = jax.nn.sigmoid(gate_pre)
        act = gate_pre * sig
        hidden_ref[...] = (act * up_pre).astype(BF16)
        act_ref[...] = act
        slope_ref[...] = up_pre * (sig * (1.0 + gate_pre * (1.0 - sig)))

    column = pl.BlockSpec((width, block), lambda i: (0, i))
    out = pl.BlockSpec((rows, block), lambda i: (0, i))
    return pl.pallas_call(
        kernel,
        grid=(n // block,),
        in_specs=[whole(p.shape) for p in pieces] + [column, column],
        out_specs=[out, out, out],
        out_shape=[jax.ShapeDtypeStruct((rows, n), t) for t in (BF16, F32, F32)],
        cost_estimate=cost(4 * rows * width * n, rows * width, 2 * width * n, 5 * rows * n),
    )(*pieces, gate_weight, up_weight)


def backward(pieces, down_weight_t, act, slope):
    width, n = down_weight_t.shape
    rows = sum(p.shape[0] for p in pieces)
    block = 256

    def kernel(a, b, c, d, e, dw, act_ref, slope_ref, gate_ref, up_ref):
        cot = jnp.concatenate([r[...] for r in (a, b, c, d, e)], axis=0)
        hid_grad = jnp.dot(cot, dw[...], preferred_element_type=F32)
        gate_ref[...] = (hid_grad * slope_ref[...]).astype(BF16)
        up_ref[...] = (hid_grad * act_ref[...]).astype(BF16)

    out = pl.BlockSpec((rows, block), lambda i: (0, i))
    return pl.pallas_call(
        kernel,
        grid=(n // block,),
        in_specs=[whole(p.shape) for p in pieces] + [pl.BlockSpec((width, block), lambda i: (0, i)), out, out],
        out_specs=[out, out],
        out_shape=[jax.ShapeDtypeStruct((rows, n), BF16)] * 2,
        cost_estimate=cost(2 * rows * width * n, rows * width, width * n, 6 * rows * n),
    )(*pieces, down_weight_t, act, slope)


def weight_grad(near, far, rhs, place, z_first):
    width, n_near = near.shape
    tokens, n_one = rhs[0].shape
    n = n_one * len(rhs)
    nz, ny = lax.axis_size("z"), lax.axis_size("y")
    rows = width // (nz * ny * 2)
    block = width // nz

    def kernel(place_ref, near_ref, far_ref, *refs):
        c, y = place_ref[0], place_ref[2]
        mine_ref, theirs_ref = refs[-2:]
        lhs = jnp.concatenate([near_ref[...], far_ref[...]], axis=1)
        for k in range(len(rhs)):
            out = jnp.dot(lhs, refs[k][...], preferred_element_type=F32).reshape(ny, 2, rows, n_one)
            first, second = out[:, 0], out[:, 1]
            mine = jnp.where(c == 0, first, second).astype(BF16)
            theirs = jnp.where(c == 0, second, first).astype(BF16)
            at = pl.ds(k * n_one, n_one)
            if z_first:
                mine_ref[0, :, :, at], theirs_ref[0, :, :, at] = mine, theirs
            else:
                for j in range(ny):
                    rel = (j + ny - y) % ny
                    mine_ref[rel, 0, :, at], theirs_ref[rel, 0, :, at] = mine[j], theirs[j]

    if z_first:
        lhs_at = lambda i, place: ((i + place[1]) % nz, 0)
        out_spec = pl.BlockSpec((1, ny, rows, n), lambda i, place: (i, 0, 0, 0))
        shape = jax.ShapeDtypeStruct((nz, ny, rows, n), BF16)
    else:
        lhs_at = lambda i, place: (i, 0)
        out_spec = pl.BlockSpec((ny, 1, rows, n), lambda i, place: (0, i, 0, 0))
        shape = jax.ShapeDtypeStruct((ny, nz, rows, n), BF16)
    return pl.pallas_call(
        kernel,
        grid_spec=pltpu.PrefetchScalarGridSpec(
            num_scalar_prefetch=1,
            grid=(nz,),
            in_specs=[
                pl.BlockSpec((block, n_near), lhs_at),
                pl.BlockSpec((block, tokens - n_near), lhs_at),
            ]
            + [whole((tokens, n_one))] * len(rhs),
            out_specs=[out_spec, out_spec],
        ),
        out_shape=[shape, shape],
        cost_estimate=cost(2 * tokens * width * n, tokens * (width + n), width * n),
    )(place, near, far, *rhs)


def input_parts(gate_back, up_back, gate_weight, up_weight, place):
    tokens, n = gate_back.shape
    width = gate_weight.shape[0]
    block = 512
    rows = tokens // 4

    def kernel(place_ref, gb, ub, gw, uw, out_ref):
        x = place_ref[3]
        part = lax.dot_general(gb[...], gw[...], NT, preferred_element_type=F32)
        part = (part + lax.dot_general(ub[...], uw[...], NT, preferred_element_type=F32)).astype(BF16)
        for k, by in enumerate((0, 3, 1, 2)):
            out_ref[(x + by) % 4] = part[k * rows : (k + 1) * rows]

    return pl.pallas_call(
        kernel,
        grid_spec=pltpu.PrefetchScalarGridSpec(
            num_scalar_prefetch=1,
            grid=(width // block,),
            in_specs=[whole((tokens, n))] * 2 + [pl.BlockSpec((block, n), lambda i, place: (i, 0))] * 2,
            out_specs=pl.BlockSpec((4, rows, block), lambda i, place: (0, 0, i)),
        ),
        out_shape=jax.ShapeDtypeStruct((4, rows, width), BF16),
        cost_estimate=cost(4 * tokens * width * n, 2 * tokens * n, 2 * width * n, tokens * width),
    )(place, gate_back, up_back, gate_weight, up_weight)


def from_partner(theirs):
    return lax.ppermute(theirs, "tp", [(0, 1), (1, 0)])


def summed_all_to_all(value, axis):
    arrived = lax.all_to_all(value, axis, split_axis=0, concat_axis=0, tiled=True)
    return arrived.astype(F32).sum(axis=0)


def over_y(mine, theirs):
    partner = from_partner(theirs)
    h = mine.shape[1] // 2
    top, bottom = slice(0, h), slice(h, None)
    far_up = shifted(total(mine[2, top], partner[2, top]).astype(BF16), "y", 1)
    far_down = shifted(total(mine[2, bottom], partner[2, bottom]).astype(BF16), "y", -1)
    up = halves(total(mine[1, top], partner[1, top], far_up), total(mine[1, bottom], partner[1, bottom]))
    down = halves(total(mine[3, top], partner[3, top]), total(mine[3, bottom], partner[3, bottom], far_down))
    up = shifted(up.astype(BF16), "y", 1)
    down = shifted(down.astype(BF16), "y", -1)
    return total(mine[0], partner[0], up, down)


def over_z(mine, theirs):
    partner = from_partner(theirs)
    h = mine.shape[1] // 2
    top, bottom = slice(0, h), slice(h, None)
    up = shifted(total(mine[4, top], partner[4, top]).astype(BF16), "z", 1)
    down = shifted(total(mine[4, bottom], partner[4, bottom]).astype(BF16), "z", -1)
    up = halves(total(mine[3, top], partner[3, top], up), total(mine[3, bottom], partner[3, bottom]))
    down = halves(total(mine[5, top], partner[5, top]), total(mine[5, bottom], partner[5, bottom], down))
    up, down = shifted(up.astype(BF16), "z", 1), shifted(down.astype(BF16), "z", -1)
    for near, far in ((2, 6), (1, 7)):
        up = shifted(total(mine[near], partner[near], up).astype(BF16), "z", 1)
        down = shifted(total(mine[far], partner[far], down).astype(BF16), "z", -1)
    return total(mine[0], partner[0], up, down)


def on_device(tokens, cotangent, gate_weight, up_weight, down_weight_t):
    n_dev = lax.axis_size("z") * lax.axis_size("y") * lax.axis_size("fs") * lax.axis_size("tp")
    scale = float(tokens.shape[0] * n_dev) ** -0.5
    place = jnp.stack([lax.axis_index(a) for a in ("tp", "z", "y", "fs")]).astype(jnp.int32)
    tok = ring_gather(tokens)
    cot = ring_gather(cotangent)
    tok_near, tok_far = turned(tok[:3]), turned(tok[3:])
    cot_near, cot_far = turned(cot[:3]), turned(cot[3:])
    hidden, act, slope = forward(tok, gate_weight, up_weight)

    mine_d, theirs_d = weight_grad(cot_near, cot_far, (hidden,), place, True)
    act, slope, mine_d = lax.optimization_barrier((act, slope, mine_d))
    gate_back, up_back = backward(cot, down_weight_t, act, slope)
    mine_g, theirs_g = weight_grad(tok_near, tok_far, (gate_back, up_back), place, False)
    gate_back, up_back, mine_g = lax.optimization_barrier((gate_back, up_back, mine_g))
    parts = input_parts(gate_back, up_back, gate_weight, up_weight, place)

    line = over_z(mine_d, theirs_d).astype(BF16)
    plane = over_y(mine_g, theirs_g).astype(BF16)
    input_grad = summed_all_to_all(parts, "fs").astype(BF16)
    down_grad = summed_all_to_all(line, "y") * scale
    both = summed_all_to_all(plane, "z") * scale
    n = gate_back.shape[1]
    return input_grad, both[:, :n], both[:, n:], down_grad


def solution(mesh):
    n_rep, n_fs, n_tp = (mesh.shape[a] for a in ("rep", "fs", "tp"))
    ny = 4
    grid = Mesh(mesh.devices.reshape(n_rep // ny, ny, n_fs, n_tp), ("z", "y", "fs", "tp"))
    split = P(("z", "y", "fs", "tp"), None)
    weight = P(None, "fs")
    grad = P(("z", "y", "tp"), "fs")
    return jax.shard_map(
        on_device,
        mesh=grid,
        in_specs=(split, split, weight, weight, weight),
        out_specs=(split, grad, grad, grad),
        check_vma=False,
    )
```

```python
import jax
import jax.numpy as jnp
from jax import lax
from jax.experimental import pallas as pl
from jax.experimental.pallas import tpu as pltpu
from jax.sharding import Mesh
from jax.sharding import PartitionSpec as P


F32 = jnp.float32
BF16 = jnp.bfloat16
NT = (((1,), (1,)), ((), ()))


def shifted(value, axis, by):
    n = lax.axis_size(axis)
    return lax.ppermute(value, axis, [(i, (i + by) % n) for i in range(n)])


def total(*values):
    return sum(v.astype(F32) for v in values)


def halves(a, b):
    return jnp.concatenate([a, b], axis=0)


def ring_gather(value):
    half = value.shape[0] // 2
    left = shifted(value, "fs", 1)
    right = shifted(value, "fs", -1)
    far_top = shifted(left[:half], "fs", 1)
    far_bottom = shifted(right[half:], "fs", -1)
    return value, left, right, far_top, far_bottom


def resident(kernel, outs, operands, place, flops, scratch=()):
    nbytes = sum(v.size * v.dtype.itemsize for v in operands)
    return pl.pallas_call(
        kernel,
        in_specs=[pl.BlockSpec(memory_space=pltpu.SMEM)] + [pl.BlockSpec(memory_space=pltpu.VMEM)] * len(operands),
        out_specs=[pl.BlockSpec(memory_space=pltpu.VMEM)] * len(outs),
        out_shape=[pltpu.VMEM(shape, dtype) for shape, dtype in outs],
        scratch_shapes=scratch,
        compiler_params=pltpu.CompilerParams(vmem_limit_bytes=12 * 2**20),
        cost_estimate=pl.CostEstimate(flops=flops, bytes_accessed=nbytes, transcendentals=0),
    )(place, *(pltpu.with_memory_space_constraint(v, pltpu.VMEM) for v in operands))


def turned(pieces, place):
    width = pieces[0].shape[1]
    rows = sum(p.shape[0] for p in pieces)
    block = 256

    def kernel(_, *refs):
        def step(i, carry):
            at = pl.ds(pl.multiple_of(i * block, block), block)
            refs[-1][at, :] = jnp.concatenate([r[:, at] for r in refs[:-1]], axis=0).T
            return carry

        lax.fori_loop(0, width // block, step, 0)

    return resident(kernel, [((width, rows), BF16)], pieces, place, 16 * rows * width)[0]


def forward(pieces, gate_weight, up_weight, place):
    width, n = gate_weight.shape
    rows = sum(p.shape[0] for p in pieces)
    block = 256

    def kernel(_, a, b, c, d, e, gw, uw, hidden_ref, act_ref, slope_ref):
        def step(i, carry):
            at = pl.ds(pl.multiple_of(i * block, block), block)
            tok = jnp.concatenate([r[...] for r in (a, b, c, d, e)], axis=0)
            gate_pre = jnp.dot(tok, gw[:, at], preferred_element_type=F32)
            up_pre = jnp.dot(tok, uw[:, at], preferred_element_type=F32)
            sig = jax.nn.sigmoid(gate_pre)
            act = gate_pre * sig
            hidden_ref[:, at] = (act * up_pre).astype(BF16)
            act_ref[:, at] = act
            slope_ref[:, at] = up_pre * (sig * (1.0 + gate_pre * (1.0 - sig)))
            return carry

        lax.fori_loop(0, n // block, step, 0)

    outs = [((rows, n), t) for t in (BF16, F32, F32)]
    return resident(kernel, outs, (*pieces, gate_weight, up_weight), place, 4 * rows * width * n)


def backward(pieces, down_weight_t, act, slope, place):
    width, n = down_weight_t.shape
    rows = sum(p.shape[0] for p in pieces)
    block = 256

    def kernel(_, a, b, c, d, e, dw, act_ref, slope_ref, gate_ref, up_ref):
        def step(i, carry):
            at = pl.ds(pl.multiple_of(i * block, block), block)
            cot = jnp.concatenate([r[...] for r in (a, b, c, d, e)], axis=0)
            hid_grad = jnp.dot(cot, dw[:, at], preferred_element_type=F32)
            gate_ref[:, at] = (hid_grad * slope_ref[:, at]).astype(BF16)
            up_ref[:, at] = (hid_grad * act_ref[:, at]).astype(BF16)
            return carry

        lax.fori_loop(0, n // block, step, 0)

    outs = [((rows, n), BF16)] * 2
    return resident(kernel, outs, (*pieces, down_weight_t, act, slope), place, 2 * rows * width * n)


def weight_grad(near, far, rhs, place, sizes, z_first):
    width, _ = near.shape
    tokens, n_one = rhs[0].shape
    n = n_one * len(rhs)
    nz, ny = sizes
    rows = width // (nz * ny * 2)
    block = width // nz

    def kernel(place_ref, near_ref, far_ref, *refs):
        c, z, y = place_ref[0], place_ref[1], place_ref[2]
        mine_ref, theirs_ref, scratch = refs[-3:]

        def step(i, carry):
            place_z = (i + z) % nz if z_first else i
            at = pl.ds(pl.multiple_of(place_z * block, block), block)
            lhs = jnp.concatenate([near_ref[at, :], far_ref[at, :]], axis=1)
            for k in range(len(rhs)):
                out = jnp.dot(lhs, refs[k][...], preferred_element_type=F32)
                scratch[...] = out.reshape(2 * ny, rows, n_one)
                for j in range(ny):
                    from_y = j if z_first else (y + j) % ny
                    to = (i, j) if z_first else (j, i)
                    cols = pl.ds(k * n_one, n_one)
                    mine_ref[(*to, slice(None), cols)] = scratch[2 * from_y + c].astype(BF16)
                    theirs_ref[(*to, slice(None), cols)] = scratch[2 * from_y + 1 - c].astype(BF16)
            return carry

        lax.fori_loop(0, nz, step, 0)

    shape = (nz, ny, rows, n) if z_first else (ny, nz, rows, n)
    scratch = [pltpu.VMEM((2 * ny, rows, n_one), F32)]
    return resident(kernel, [(shape, BF16)] * 2, (near, far, *rhs), place, 2 * tokens * width * n, scratch)


def input_parts(gate_back, up_back, gate_weight, up_weight, place):
    tokens, n = gate_back.shape
    width = gate_weight.shape[0]
    block = 256
    rows = tokens // 4

    def kernel(place_ref, gb, ub, gw, uw, out_ref):
        x = place_ref[3]

        def step(i, carry):
            at = pl.ds(pl.multiple_of(i * block, block), block)
            part = lax.dot_general(gb[...], gw[at, :], NT, preferred_element_type=F32)
            part = (part + lax.dot_general(ub[...], uw[at, :], NT, preferred_element_type=F32)).astype(BF16)
            for k, by in enumerate((0, 3, 1, 2)):
                out_ref[(x + by) % 4, :, at] = part[k * rows : (k + 1) * rows]
            return carry

        lax.fori_loop(0, width // block, step, 0)

    operands = (gate_back, up_back, gate_weight, up_weight)
    return resident(kernel, [((4, rows, width), BF16)], operands, place, 4 * tokens * width * n)[0]


def from_partner(theirs):
    return lax.ppermute(theirs, "tp", [(0, 1), (1, 0)])


def summed_all_to_all(value, axis):
    arrived = lax.all_to_all(value, axis, split_axis=0, concat_axis=0, tiled=True)
    return arrived.astype(F32).sum(axis=0)


def over_y(mine, theirs):
    partner = from_partner(theirs)
    h = mine.shape[1] // 2
    top, bottom = slice(0, h), slice(h, None)
    far_up = shifted(total(mine[2, top], partner[2, top]).astype(BF16), "y", 1)
    far_down = shifted(total(mine[2, bottom], partner[2, bottom]).astype(BF16), "y", -1)
    up = halves(total(mine[1, top], partner[1, top], far_up), total(mine[1, bottom], partner[1, bottom]))
    down = halves(total(mine[3, top], partner[3, top]), total(mine[3, bottom], partner[3, bottom], far_down))
    up = shifted(up.astype(BF16), "y", 1)
    down = shifted(down.astype(BF16), "y", -1)
    return total(mine[0], partner[0], up, down)


def over_z(mine, theirs):
    partner = from_partner(theirs)
    h = mine.shape[1] // 2
    top, bottom = slice(0, h), slice(h, None)
    up = shifted(total(mine[4, top], partner[4, top]).astype(BF16), "z", 1)
    down = shifted(total(mine[4, bottom], partner[4, bottom]).astype(BF16), "z", -1)
    up = halves(total(mine[3, top], partner[3, top], up), total(mine[3, bottom], partner[3, bottom]))
    down = halves(total(mine[5, top], partner[5, top]), total(mine[5, bottom], partner[5, bottom], down))
    up, down = shifted(up.astype(BF16), "z", 1), shifted(down.astype(BF16), "z", -1)
    for near, far in ((2, 6), (1, 7)):
        up = shifted(total(mine[near], partner[near], up).astype(BF16), "z", 1)
        down = shifted(total(mine[far], partner[far], down).astype(BF16), "z", -1)
    return total(mine[0], partner[0], up, down)


def on_device(tokens, cotangent, gate_weight, up_weight, down_weight_t):
    n_dev = lax.axis_size("z") * lax.axis_size("y") * lax.axis_size("fs") * lax.axis_size("tp")
    scale = float(tokens.shape[0] * n_dev) ** -0.5
    place = jnp.stack([lax.axis_index(a) for a in ("tp", "z", "y", "fs")]).astype(jnp.int32)
    sizes = lax.axis_size("z"), lax.axis_size("y")
    tok = ring_gather(tokens)
    cot = ring_gather(cotangent)
    tok_near, tok_far = turned(tok[:3], place), turned(tok[3:], place)
    cot_near, cot_far = turned(cot[:3], place), turned(cot[3:], place)
    hidden, act, slope = forward(tok, gate_weight, up_weight, place)

    mine_d, theirs_d = weight_grad(cot_near, cot_far, (hidden,), place, sizes, True)
    act, slope, mine_d = lax.optimization_barrier((act, slope, mine_d))
    gate_back, up_back = backward(cot, down_weight_t, act, slope, place)
    mine_g, theirs_g = weight_grad(tok_near, tok_far, (gate_back, up_back), place, sizes, False)
    gate_back, up_back, mine_g = lax.optimization_barrier((gate_back, up_back, mine_g))
    parts = input_parts(gate_back, up_back, gate_weight, up_weight, place)

    line = over_z(mine_d, theirs_d).astype(BF16)
    plane = over_y(mine_g, theirs_g).astype(BF16)
    input_grad = summed_all_to_all(parts, "fs").astype(BF16)
    down_grad = summed_all_to_all(line, "y") * scale
    both = summed_all_to_all(plane, "z") * scale
    n = gate_back.shape[1]
    return input_grad, both[:, :n], both[:, n:], down_grad


def solution(mesh):
    n_rep, n_fs, n_tp = (mesh.shape[a] for a in ("rep", "fs", "tp"))
    ny = 4
    grid = Mesh(mesh.devices.reshape(n_rep // ny, ny, n_fs, n_tp), ("z", "y", "fs", "tp"))
    split = P(("z", "y", "fs", "tp"), None)
    weight = P(None, "fs")
    grad = P(("z", "y", "tp"), "fs")
    return jax.shard_map(
        on_device,
        mesh=grid,
        in_specs=(split, split, weight, weight, weight),
        out_specs=(split, grad, grad, grad),
        check_vma=False,
    )
```

```python
import jax
import jax.numpy as jnp
from jax import lax
from jax.experimental import pallas as pl
from jax.experimental.pallas import tpu as pltpu
from jax.sharding import Mesh
from jax.sharding import PartitionSpec as P


F32 = jnp.float32
BF16 = jnp.bfloat16
NT = (((1,), (1,)), ((), ()))


def onward(value, axis):
    n = lax.axis_size(axis)
    return lax.ppermute(value, (axis, "tp"), [(2 * i + c, 2 * ((i + 1 - 2 * c) % n) + c) for i in range(n) for c in range(2)])


def total(*values):
    return sum(v.astype(F32) for v in values)


def ring_gather(value):
    pieces = [value]
    for _ in range(1, 4):
        pieces.append(onward(pieces[-1], "fs"))
    return pieces


def ring_sum(terms, axis):
    value = total(*terms[-1])
    for k in range(len(terms) - 2, -1, -1):
        value = total(*terms[k], onward(value.astype(BF16), axis))
    return value


def resident(kernel, outs, operands, place, flops, scratch=()):
    nbytes = sum(v.size * v.dtype.itemsize for v in operands)
    return pl.pallas_call(
        kernel,
        in_specs=[pl.BlockSpec(memory_space=pltpu.SMEM)] + [pl.BlockSpec(memory_space=pltpu.VMEM)] * len(operands),
        out_specs=[pl.BlockSpec(memory_space=pltpu.VMEM)] * len(outs),
        out_shape=[pltpu.VMEM(shape, dtype) for shape, dtype in outs],
        scratch_shapes=scratch,
        compiler_params=pltpu.CompilerParams(vmem_limit_bytes=12 * 2**20),
        cost_estimate=pl.CostEstimate(flops=flops, bytes_accessed=nbytes, transcendentals=0),
    )(place, *(pltpu.with_memory_space_constraint(v, pltpu.VMEM) for v in operands))


def turned(pieces, place):
    width = pieces[0].shape[1]
    rows = sum(p.shape[0] for p in pieces)
    block = 256

    def kernel(_, *refs):
        def step(i, carry):
            at = pl.ds(pl.multiple_of(i * block, block), block)
            refs[-1][at, :] = jnp.concatenate([r[:, at] for r in refs[:-1]], axis=0).T
            return carry

        lax.fori_loop(0, width // block, step, 0)

    return resident(kernel, [((width, rows), BF16)], pieces, place, 16 * rows * width)[0]


def forward(pieces, gate_weight, up_weight, place):
    width, n = gate_weight.shape
    rows = sum(p.shape[0] for p in pieces)
    block = 256

    def kernel(_, a, b, c, d, gw, uw, hidden_ref, act_ref, slope_ref):
        def step(i, carry):
            at = pl.ds(pl.multiple_of(i * block, block), block)
            tok = jnp.concatenate([r[...] for r in (a, b, c, d)], axis=0)
            gate_pre = jnp.dot(tok, gw[:, at], preferred_element_type=F32)
            up_pre = jnp.dot(tok, uw[:, at], preferred_element_type=F32)
            sig = jax.nn.sigmoid(gate_pre)
            act = gate_pre * sig
            hidden_ref[:, at] = (act * up_pre).astype(BF16)
            act_ref[:, at] = act
            slope_ref[:, at] = up_pre * (sig * (1.0 + gate_pre * (1.0 - sig)))
            return carry

        lax.fori_loop(0, n // block, step, 0)

    outs = [((rows, n), t) for t in (BF16, F32, F32)]
    return resident(kernel, outs, (*pieces, gate_weight, up_weight), place, 4 * rows * width * n)


def backward(pieces, down_weight_t, act, slope, place):
    width, n = down_weight_t.shape
    rows = sum(p.shape[0] for p in pieces)
    block = 256

    def kernel(_, a, b, c, d, dw, act_ref, slope_ref, gate_ref, up_ref):
        def step(i, carry):
            at = pl.ds(pl.multiple_of(i * block, block), block)
            cot = jnp.concatenate([r[...] for r in (a, b, c, d)], axis=0)
            hid_grad = jnp.dot(cot, dw[:, at], preferred_element_type=F32)
            gate_ref[:, at] = (hid_grad * slope_ref[:, at]).astype(BF16)
            up_ref[:, at] = (hid_grad * act_ref[:, at]).astype(BF16)
            return carry

        lax.fori_loop(0, n // block, step, 0)

    outs = [((rows, n), BF16)] * 2
    return resident(kernel, outs, (*pieces, down_weight_t, act, slope), place, 2 * rows * width * n)


def weight_grad(near, far, rhs, place, sizes, z_first):
    width, _ = near.shape
    tokens, n = rhs.shape
    nz, ny = sizes
    rows = width // (nz * ny * 2)
    block = 2 * width // nz

    def kernel(place_ref, near_ref, far_ref, rhs_ref, mine_ref, theirs_ref):
        c, z, y = place_ref[0], place_ref[1], place_ref[2]
        way = 1 - 2 * c

        def step(i, carry):
            at = pl.ds(pl.multiple_of(i * block, block), block)
            lhs = jnp.concatenate([near_ref[at, :], far_ref[at, :]], axis=1)
            out = jnp.dot(lhs, rhs_ref[...], preferred_element_type=F32).reshape(2, ny, 2, rows, n)
            mine = jnp.where(c == 0, out[:, :, 0], out[:, :, 1]).astype(BF16)
            theirs = jnp.where(c == 0, out[:, :, 1], out[:, :, 0]).astype(BF16)
            for k in range(2):
                for j in range(ny):
                    up_z, up_y = (way * (2 * i + k - z) + 2 * nz) % nz, (way * (j - y) + 2 * ny) % ny
                    down_z, down_y = (nz - up_z) % nz, (ny - up_y) % ny
                    if z_first:
                        mine_ref[up_z, up_y], theirs_ref[down_z, down_y] = mine[k, j], theirs[k, j]
                    else:
                        mine_ref[up_y, up_z], theirs_ref[down_y, down_z] = mine[k, j], theirs[k, j]
            return carry

        lax.fori_loop(0, nz // 2, step, 0)

    shape = (nz, ny, rows, n) if z_first else (ny, nz, rows, n)
    return resident(kernel, [(shape, BF16)] * 2, (near, far, rhs), place, 2 * tokens * width * n)


def input_parts(gate_back, up_back, gate_weight, up_weight, place):
    tokens, n = gate_back.shape
    width = gate_weight.shape[0]
    block = 256
    rows = tokens // 4

    def kernel(_, gb, ub, gw, uw, *outs):
        def step(i, carry):
            at = pl.ds(pl.multiple_of(i * block, block), block)
            part = lax.dot_general(gb[...], gw[at, :], NT, preferred_element_type=F32)
            part = (part + lax.dot_general(ub[...], uw[at, :], NT, preferred_element_type=F32)).astype(BF16)
            for k in range(4):
                outs[(4 - k) % 4][:, at] = part[k * rows : (k + 1) * rows]
            return carry

        lax.fori_loop(0, width // block, step, 0)

    operands = (gate_back, up_back, gate_weight, up_weight)
    return resident(kernel, [((rows, width), BF16)] * 4, operands, place, 4 * tokens * width * n)


def with_partner(mine, theirs):
    partner = lax.ppermute(theirs, "tp", [(0, 1), (1, 0)])
    return [(mine[k], partner[k]) for k in range(mine.shape[0])]


def on_device(tokens, cotangent, gate_weight, up_weight, down_weight_t):
    sizes = lax.axis_size("z"), lax.axis_size("y")
    n_dev = sizes[0] * sizes[1] * lax.axis_size("fs") * lax.axis_size("tp")
    scale = float(tokens.shape[0] * n_dev) ** -0.5
    place = jnp.stack([lax.axis_index(a) for a in ("tp", "z", "y")]).astype(jnp.int32)
    tok = ring_gather(tokens)
    cot = ring_gather(cotangent)
    tok_near, tok_far = turned(tok[:3], place), turned(tok[3:], place)
    cot_near, cot_far = turned(cot[:3], place), turned(cot[3:], place)
    hidden, act, slope = forward(tok, gate_weight, up_weight, place)

    mine_d, theirs_d = weight_grad(cot_near, cot_far, hidden, place, sizes, False)
    act, slope, mine_d = lax.optimization_barrier((act, slope, mine_d))
    gate_back, up_back = backward(cot, down_weight_t, act, slope, place)
    mine_g, theirs_g = weight_grad(tok_near, tok_far, gate_back, place, sizes, False)
    up_late, mine_g = lax.optimization_barrier((up_back, mine_g))
    mine_u, theirs_u = weight_grad(tok_near, tok_far, up_late, place, sizes, True)
    gate_late, up_late, mine_u = lax.optimization_barrier((gate_back, up_late, mine_u))
    parts = input_parts(gate_late, up_late, gate_weight, up_weight, place)

    plane_d = ring_sum(with_partner(mine_d, theirs_d), "y").astype(BF16)
    plane_g = ring_sum(with_partner(mine_g, theirs_g), "y").astype(BF16)
    line_u = ring_sum(with_partner(mine_u, theirs_u), "z").astype(BF16)
    input_grad = ring_sum([(p,) for p in parts], "fs").astype(BF16)
    both = jnp.concatenate([plane_g, plane_d], axis=2)
    both = ring_sum([(both[k],) for k in range(sizes[0])], "z") * scale
    up_grad = ring_sum([(line_u[k],) for k in range(sizes[1])], "y") * scale
    n = gate_back.shape[1]
    return input_grad, both[:, :n], up_grad, both[:, n:]


def solution(mesh):
    n_rep, n_fs, n_tp = (mesh.shape[a] for a in ("rep", "fs", "tp"))
    ny = 4
    grid = Mesh(mesh.devices.reshape(n_rep // ny, ny, n_fs, n_tp), ("z", "y", "fs", "tp"))
    split = P(("z", "y", "fs", "tp"), None)
    weight = P(None, "fs")
    grad = P(("z", "y", "tp"), "fs")
    return jax.shard_map(
        on_device,
        mesh=grid,
        in_specs=(split, split, weight, weight, weight),
        out_specs=(split, grad, grad, grad),
        check_vma=False,
    )
```

```python
import jax
import jax.numpy as jnp
from jax import lax
from jax.experimental import pallas as pl
from jax.experimental.pallas import tpu as pltpu
from jax.sharding import Mesh
from jax.sharding import PartitionSpec as P


F32 = jnp.float32
BF16 = jnp.bfloat16
NT = (((1,), (1,)), ((), ()))


def onward(value, axis, stride=1):
    n = lax.axis_size(axis)
    return lax.ppermute(value, (axis, "tp"), [(2 * i + c, 2 * ((i + stride * (1 - 2 * c)) % n) + c) for i in range(n) for c in range(2)])


def total(*values):
    return sum(v.astype(F32) for v in values)


def ring_gather(value):
    pieces = [value]
    for _ in range(1, 4):
        pieces.append(onward(pieces[-1], "fs"))
    return pieces


def ring_sum(parts, axis, stride=1):
    n = parts[0].shape[0]
    value = total(*(p[n - 1] for p in parts))
    for k in range(n - 2, -1, -1):
        value = total(*(p[k] for p in parts), onward(value.astype(BF16), axis, stride))
    return value


def ring_sum_of(pieces, axis):
    value = pieces[-1]
    for k in range(len(pieces) - 2, -1, -1):
        value = total(pieces[k], onward(value.astype(BF16), axis))
    return value


def pair_place(owner, me, core, n):
    side = 1 - 2 * ((me + core) % 2)
    away = owner - me + n
    other = away % 2
    return other * (n // 2) + ((1 - 2 * core) * (away - other * side) + 4 * n) % n // 2


def pair_sum(parts, axis):
    n = parts[0].shape[0]
    perm = [(2 * i + c, 2 * ((i + 1 - 2 * ((i + c) % 2)) % n) + c) for i in range(n) for c in range(2)]
    value = total(*(p[n // 2 :] for p in parts)).astype(BF16)
    arrived = lax.ppermute(value, (axis, "tp"), perm)
    return ring_sum([p[: n // 2] for p in parts] + [arrived], axis, 2)


def resident(kernel, outs, operands, place, flops, scratch=()):
    nbytes = sum(v.size * v.dtype.itemsize for v in operands)
    return pl.pallas_call(
        kernel,
        in_specs=[pl.BlockSpec(memory_space=pltpu.SMEM)] + [pl.BlockSpec(memory_space=pltpu.VMEM)] * len(operands),
        out_specs=[pl.BlockSpec(memory_space=pltpu.VMEM)] * len(outs),
        out_shape=[pltpu.VMEM(shape, dtype) for shape, dtype in outs],
        scratch_shapes=scratch,
        compiler_params=pltpu.CompilerParams(vmem_limit_bytes=12 * 2**20),
        cost_estimate=pl.CostEstimate(flops=flops, bytes_accessed=nbytes, transcendentals=0),
    )(place, *(pltpu.with_memory_space_constraint(v, pltpu.VMEM) for v in operands))


def turned(pieces, place):
    width = pieces[0].shape[1]
    rows = sum(p.shape[0] for p in pieces)
    block = 256

    def kernel(_, *refs):
        def step(i, carry):
            at = pl.ds(pl.multiple_of(i * block, block), block)
            refs[-1][at, :] = jnp.concatenate([r[:, at] for r in refs[:-1]], axis=0).T
            return carry

        lax.fori_loop(0, width // block, step, 0)

    return resident(kernel, [((width, rows), BF16)], pieces, place, 16 * rows * width)[0]


def forward(pieces, gate_weight, up_weight, place):
    width, n = gate_weight.shape
    rows = sum(p.shape[0] for p in pieces)
    block = 256

    def kernel(_, a, b, c, d, gw, uw, hidden_ref, act_ref, slope_ref):
        def step(i, carry):
            at = pl.ds(pl.multiple_of(i * block, block), block)
            tok = jnp.concatenate([r[...] for r in (a, b, c, d)], axis=0)
            gate_pre = jnp.dot(tok, gw[:, at], preferred_element_type=F32)
            up_pre = jnp.dot(tok, uw[:, at], preferred_element_type=F32)
            sig = jax.nn.sigmoid(gate_pre)
            act = gate_pre * sig
            hidden_ref[:, at] = (act * up_pre).astype(BF16)
            act_ref[:, at] = act
            slope_ref[:, at] = up_pre * (sig * (1.0 + gate_pre * (1.0 - sig)))
            return carry

        lax.fori_loop(0, n // block, step, 0)

    outs = [((rows, n), t) for t in (BF16, F32, F32)]
    return resident(kernel, outs, (*pieces, gate_weight, up_weight), place, 4 * rows * width * n)


def backward(pieces, down_weight_t, act, slope, place):
    width, n = down_weight_t.shape
    rows = sum(p.shape[0] for p in pieces)
    block = 256

    def kernel(_, a, b, c, d, dw, act_ref, slope_ref, gate_ref, up_ref):
        def step(i, carry):
            at = pl.ds(pl.multiple_of(i * block, block), block)
            cot = jnp.concatenate([r[...] for r in (a, b, c, d)], axis=0)
            hid_grad = jnp.dot(cot, dw[:, at], preferred_element_type=F32)
            gate_ref[:, at] = (hid_grad * slope_ref[:, at]).astype(BF16)
            up_ref[:, at] = (hid_grad * act_ref[:, at]).astype(BF16)
            return carry

        lax.fori_loop(0, n // block, step, 0)

    outs = [((rows, n), BF16)] * 2
    return resident(kernel, outs, (*pieces, down_weight_t, act, slope), place, 2 * rows * width * n)


def weight_grad(near, far, rhs, place, sizes, z_first):
    width, _ = near.shape
    tokens, n = rhs.shape
    nz, ny = sizes
    rows = width // (nz * ny * 2)
    block = 2 * width // nz

    def kernel(place_ref, near_ref, far_ref, rhs_ref, mine_ref, theirs_ref):
        c, z, y = place_ref[0], place_ref[1], place_ref[2]
        way = 1 - 2 * c

        def step(i, carry):
            at = pl.ds(pl.multiple_of(i * block, block), block)
            lhs = jnp.concatenate([near_ref[at, :], far_ref[at, :]], axis=1)
            out = jnp.dot(lhs, rhs_ref[...], preferred_element_type=F32).reshape(2, ny, 2, rows, n)
            mine = jnp.where(c == 0, out[:, :, 0], out[:, :, 1]).astype(BF16)
            theirs = jnp.where(c == 0, out[:, :, 1], out[:, :, 0]).astype(BF16)
            for k in range(2):
                at_z = 2 * i + k
                mine_z, theirs_z = pair_place(at_z, z, c, nz), pair_place(at_z, z, 1 - c, nz)
                for j in range(ny):
                    if z_first:
                        mine_y, theirs_y = pair_place(j, y, c, ny), pair_place(j, y, 1 - c, ny)
                        mine_ref[mine_z, mine_y], theirs_ref[theirs_z, theirs_y] = mine[k, j], theirs[k, j]
                    else:
                        mine_y = (way * (j - y) + 2 * ny) % ny
                        theirs_y = (ny - mine_y) % ny
                        mine_ref[mine_y, mine_z], theirs_ref[theirs_y, theirs_z] = mine[k, j], theirs[k, j]
            return carry

        lax.fori_loop(0, nz // 2, step, 0)

    shape = (nz, ny, rows, n) if z_first else (ny, nz, rows, n)
    return resident(kernel, [(shape, BF16)] * 2, (near, far, rhs), place, 2 * tokens * width * n)


def input_parts(gate_back, up_back, gate_weight, up_weight, place):
    tokens, n = gate_back.shape
    width = gate_weight.shape[0]
    block = 256
    rows = tokens // 4

    def kernel(_, gb, ub, gw, uw, *outs):
        def step(i, carry):
            at = pl.ds(pl.multiple_of(i * block, block), block)
            part = lax.dot_general(gb[...], gw[at, :], NT, preferred_element_type=F32)
            part = (part + lax.dot_general(ub[...], uw[at, :], NT, preferred_element_type=F32)).astype(BF16)
            for k in range(4):
                outs[(4 - k) % 4][:, at] = part[k * rows : (k + 1) * rows]
            return carry

        lax.fori_loop(0, width // block, step, 0)

    operands = (gate_back, up_back, gate_weight, up_weight)
    return resident(kernel, [((rows, width), BF16)] * 4, operands, place, 4 * tokens * width * n)


def with_partner(mine, theirs):
    return mine, lax.ppermute(theirs, "tp", [(0, 1), (1, 0)])


def on_device(tokens, cotangent, gate_weight, up_weight, down_weight_t):
    sizes = lax.axis_size("z"), lax.axis_size("y")
    n_dev = sizes[0] * sizes[1] * lax.axis_size("fs") * lax.axis_size("tp")
    scale = float(tokens.shape[0] * n_dev) ** -0.5
    place = jnp.stack([lax.axis_index(a) for a in ("tp", "z", "y")]).astype(jnp.int32)
    tok = ring_gather(tokens)
    cot = ring_gather(cotangent)
    tok_near, tok_far = turned(tok[:3], place), turned(tok[3:], place)
    cot_near, cot_far = turned(cot[:3], place), turned(cot[3:], place)
    hidden, act, slope = forward(tok, gate_weight, up_weight, place)

    mine_d, theirs_d = weight_grad(cot_near, cot_far, hidden, place, sizes, False)
    act, slope, mine_d = lax.optimization_barrier((act, slope, mine_d))
    gate_back, up_back = backward(cot, down_weight_t, act, slope, place)
    mine_g, theirs_g = weight_grad(tok_near, tok_far, gate_back, place, sizes, False)
    up_late, mine_g = lax.optimization_barrier((up_back, mine_g))
    mine_u, theirs_u = weight_grad(tok_near, tok_far, up_late, place, sizes, True)
    gate_late, up_late, mine_u = lax.optimization_barrier((gate_back, up_late, mine_u))
    parts = input_parts(gate_late, up_late, gate_weight, up_weight, place)

    plane_d = ring_sum(with_partner(mine_d, theirs_d), "y").astype(BF16)
    plane_g = ring_sum(with_partner(mine_g, theirs_g), "y").astype(BF16)
    line_u = pair_sum(with_partner(mine_u, theirs_u), "z").astype(BF16)
    input_grad = ring_sum_of(parts, "fs").astype(BF16)
    both = jnp.concatenate([plane_g, plane_d], axis=2)
    both = pair_sum([both], "z") * scale
    up_grad = pair_sum([line_u], "y") * scale
    n = gate_back.shape[1]
    return input_grad, both[:, :n], up_grad, both[:, n:]


def solution(mesh):
    n_rep, n_fs, n_tp = (mesh.shape[a] for a in ("rep", "fs", "tp"))
    ny = 4
    grid = Mesh(mesh.devices.reshape(n_rep // ny, ny, n_fs, n_tp), ("z", "y", "fs", "tp"))
    split = P(("z", "y", "fs", "tp"), None)
    weight = P(None, "fs")
    grad = P(("z", "y", "tp"), "fs")
    return jax.shard_map(
        on_device,
        mesh=grid,
        in_specs=(split, split, weight, weight, weight),
        out_specs=(split, grad, grad, grad),
        check_vma=False,
    )
```

```python
import jax
import jax.numpy as jnp
from jax import lax
from jax.experimental import pallas as pl
from jax.experimental.pallas import tpu as pltpu
from jax.sharding import Mesh
from jax.sharding import PartitionSpec as P


F32 = jnp.float32
BF16 = jnp.bfloat16
NT = (((1,), (1,)), ((), ()))


def onward(value, axis, stride=1):
    n = lax.axis_size(axis)
    return lax.ppermute(value, (axis, "tp"), [(2 * i + c, 2 * ((i + stride * (1 - 2 * c)) % n) + c) for i in range(n) for c in range(2)])


def total(*values):
    return sum(v.astype(F32) for v in values)


def ring_gather(value):
    pieces = [value]
    for _ in range(1, 4):
        pieces.append(onward(pieces[-1], "fs"))
    return pieces


def ring_sum(parts, axis, stride=1):
    arrived = ()
    for k in range(len(parts) - 1, -1, -1):
        value = total(*parts[k], *arrived)
        value = value.astype(BF16) if k else value
        arrived = (onward(value, axis, stride),) if k else ()
    return value


def pair_place(owner, me, core, n):
    side = 1 - 2 * ((me + core) % 2)
    away = owner - me + n
    other = away % 2
    return other * (n // 2) + ((1 - 2 * core) * (away - other * side) + 4 * n) % n // 2


def pair_sum(parts, axis):
    n = parts[0].shape[0]
    perm = [(2 * i + c, 2 * ((i + 1 - 2 * ((i + c) % 2)) % n) + c) for i in range(n) for c in range(2)]
    value = total(*(p[n // 2 :] for p in parts)).astype(BF16)
    arrived = lax.ppermute(value, (axis, "tp"), perm)
    return direct_sum([tuple(p[k] for p in (*parts, arrived)) for k in range(n // 2)], axis, 2)


def direct_sum(parts, axis, stride):
    arrived = []
    for k in range(1, len(parts)):
        value = total(*parts[k]).astype(BF16)
        arrived.append(onward(value, axis, stride * k))
    return total(*parts[0], *arrived)


def resident(kernel, outs, operands, place, flops, scratch=()):
    nbytes = sum(v.size * v.dtype.itemsize for v in operands)
    return pl.pallas_call(
        kernel,
        in_specs=[pl.BlockSpec(memory_space=pltpu.SMEM)] + [pl.BlockSpec(memory_space=pltpu.VMEM)] * len(operands),
        out_specs=[pl.BlockSpec(memory_space=pltpu.VMEM)] * len(outs),
        out_shape=[pltpu.VMEM(shape, dtype) for shape, dtype in outs],
        scratch_shapes=scratch,
        compiler_params=pltpu.CompilerParams(vmem_limit_bytes=12 * 2**20),
        cost_estimate=pl.CostEstimate(flops=flops, bytes_accessed=nbytes, transcendentals=0),
    )(place, *(pltpu.with_memory_space_constraint(v, pltpu.VMEM) for v in operands))


def turned(pieces, place):
    width = pieces[0].shape[1]
    rows = sum(p.shape[0] for p in pieces)
    block = 256

    def kernel(_, *refs):
        def step(i, carry):
            at = pl.ds(pl.multiple_of(i * block, block), block)
            refs[-1][at, :] = jnp.concatenate([r[:, at] for r in refs[:-1]], axis=0).T
            return carry

        lax.fori_loop(0, width // block, step, 0)

    return resident(kernel, [((width, rows), BF16)], pieces, place, 16 * rows * width)[0]


def forward(pieces, gate_weight, up_weight, place):
    width, n = gate_weight.shape
    rows = sum(p.shape[0] for p in pieces)
    block = 256

    def kernel(_, *refs):
        gw, uw, hidden_ref, act_ref, slope_ref = refs[-5:]

        def step(i, carry):
            at = pl.ds(pl.multiple_of(i * block, block), block)
            tok = jnp.concatenate([r[...] for r in refs[:-5]], axis=0)
            gate_pre = jnp.dot(tok, gw[:, at], preferred_element_type=F32)
            up_pre = jnp.dot(tok, uw[:, at], preferred_element_type=F32)
            sig = jax.nn.sigmoid(gate_pre)
            act = gate_pre * sig
            hidden_ref[:, at] = (act * up_pre).astype(BF16)
            act_ref[:, at] = act
            slope_ref[:, at] = up_pre * (sig * (1.0 + gate_pre * (1.0 - sig)))
            return carry

        lax.fori_loop(0, n // block, step, 0)

    outs = [((rows, n), t) for t in (BF16, F32, F32)]
    return resident(kernel, outs, (*pieces, gate_weight, up_weight), place, 4 * rows * width * n)


def backward(pieces, down_weight_t, act, slope, place):
    width, n = down_weight_t.shape
    rows = sum(p.shape[0] for p in pieces)
    block = 256

    def kernel(_, *refs):
        dw, act_ref, slope_ref, gate_ref, up_ref = refs[-5:]

        def step(i, carry):
            at = pl.ds(pl.multiple_of(i * block, block), block)
            cot = jnp.concatenate([r[...] for r in refs[:-5]], axis=0)
            hid_grad = jnp.dot(cot, dw[:, at], preferred_element_type=F32)
            gate_ref[:, at] = (hid_grad * slope_ref[:, at]).astype(BF16)
            up_ref[:, at] = (hid_grad * act_ref[:, at]).astype(BF16)
            return carry

        lax.fori_loop(0, n // block, step, 0)

    outs = [((rows, n), BF16)] * 2
    return resident(kernel, outs, (*pieces, down_weight_t, act, slope), place, 2 * rows * width * n)


def weight_grad(near, far, rhs, place, sizes, z_first):
    width = near.shape[0]
    tokens, n = near.shape[1] + far.shape[1], rhs[0].shape[1]
    nz, ny = sizes
    rows = width // (nz * ny * 2)
    block = 2 * width // nz

    def kernel(place_ref, near_ref, far_ref, *refs):
        mine_ref, theirs_ref = refs[-2:]
        c, z, y = place_ref[0], place_ref[1], place_ref[2]
        way = 1 - 2 * c

        def step(i, carry):
            at = pl.ds(pl.multiple_of(i * block, block), block)
            lhs = jnp.concatenate([near_ref[at, :], far_ref[at, :]], axis=1)
            rhs = jnp.concatenate([r[...] for r in refs[:-2]], axis=0)
            out = jnp.dot(lhs, rhs, preferred_element_type=F32).reshape(2, ny, 2, rows, n)
            mine = jnp.where(c == 0, out[:, :, 0], out[:, :, 1]).astype(BF16)
            theirs = jnp.where(c == 0, out[:, :, 1], out[:, :, 0]).astype(BF16)
            for k in range(2):
                at_z = 2 * i + k
                mine_z, theirs_z = pair_place(at_z, z, c, nz), pair_place(at_z, z, 1 - c, nz)
                for j in range(ny):
                    mine_y = (way * (j - y) + 2 * ny) % ny
                    theirs_y = (ny - mine_y) % ny
                    if z_first:
                        mine_ref[mine_z, mine_y], theirs_ref[theirs_z, theirs_y] = mine[k, j], theirs[k, j]
                    else:
                        mine_ref[mine_y, mine_z], theirs_ref[theirs_y, theirs_z] = mine[k, j], theirs[k, j]
            return carry

        lax.fori_loop(0, nz // 2, step, 0)

    shape = (nz, ny, rows, n) if z_first else (ny, nz, rows, n)
    return resident(kernel, [(shape, BF16)] * 2, (near, far, *rhs), place, 2 * tokens * width * n)


def input_parts(gate_back, up_back, gate_weight, up_weight, place):
    n = gate_weight.shape[1]
    tokens = sum(v.shape[0] for v in gate_back)
    width = gate_weight.shape[0]
    block = 256
    rows = tokens // 4

    def kernel(_, *refs):
        (gw, uw), outs = refs[8:10], refs[10:]

        def step(i, carry):
            gb = jnp.concatenate([r[...] for r in refs[:4]], axis=0)
            ub = jnp.concatenate([r[...] for r in refs[4:8]], axis=0)
            at = pl.ds(pl.multiple_of(i * block, block), block)
            part = lax.dot_general(gb, gw[at, :], NT, preferred_element_type=F32)
            part = (part + lax.dot_general(ub, uw[at, :], NT, preferred_element_type=F32)).astype(BF16)
            for k in range(4):
                outs[(4 - k) % 4][:, at] = part[k * rows : (k + 1) * rows]
            return carry

        lax.fori_loop(0, width // block, step, 0)

    operands = (*gate_back, *up_back, gate_weight, up_weight)
    return resident(kernel, [((rows, width), BF16)] * 4, operands, place, 4 * tokens * width * n)


def with_partner(mine, theirs):
    return mine, lax.ppermute(theirs, "tp", [(0, 1), (1, 0)])


def by_place(parts):
    return [tuple(p[k] for p in parts) for k in range(parts[0].shape[0])]


def on_device(tokens, cotangent, gate_weight, up_weight, down_weight_t):
    sizes = lax.axis_size("z"), lax.axis_size("y")
    n_dev = sizes[0] * sizes[1] * lax.axis_size("fs") * lax.axis_size("tp")
    scale = float(tokens.shape[0] * n_dev) ** -0.5
    place = jnp.stack([lax.axis_index(a) for a in ("tp", "z", "y")]).astype(jnp.int32)
    tok = ring_gather(tokens)
    cot = ring_gather(cotangent)
    tok_near, tok_far = turned(tok[:3], place), turned(tok[3:], place)
    cot_near, cot_far = turned(cot[:3], place), turned(cot[3:], place)
    hidden, gate_back, up_back = [], [], []
    for k in range(4):
        hid, act, slope = forward(tok[k : k + 1], gate_weight, up_weight, place)
        gate, up = backward(cot[k : k + 1], down_weight_t, act, slope, place)
        hidden.append(hid)
        gate_back.append(gate)
        up_back.append(up)

    mine_g, theirs_g = weight_grad(tok_near, tok_far, gate_back, place, sizes, False)
    hidden[3], mine_g = lax.optimization_barrier((hidden[3], mine_g))
    mine_d, theirs_d = weight_grad(cot_near, cot_far, hidden, place, sizes, False)
    up_back[3], mine_d = lax.optimization_barrier((up_back[3], mine_d))
    mine_u, theirs_u = weight_grad(tok_near, tok_far, up_back, place, sizes, True)
    gate_back[3], up_back[3], mine_u = lax.optimization_barrier((gate_back[3], up_back[3], mine_u))
    parts = input_parts(gate_back, up_back, gate_weight, up_weight, place)

    plane_d = ring_sum(by_place(with_partner(mine_d, theirs_d)), "y").astype(BF16)
    plane_g = ring_sum(by_place(with_partner(mine_g, theirs_g)), "y").astype(BF16)
    line_u = pair_sum(with_partner(mine_u, theirs_u), "z").astype(BF16)
    input_grad = ring_sum([(p,) for p in parts], "fs").astype(BF16)
    both = jnp.concatenate([plane_g, plane_d], axis=2)
    both = pair_sum([both], "z") * scale
    up_grad = direct_sum(by_place([line_u]), "y", 1) * scale
    n = gate_weight.shape[1]
    return input_grad, both[:, :n], up_grad, both[:, n:]


def solution(mesh):
    n_rep, n_fs, n_tp = (mesh.shape[a] for a in ("rep", "fs", "tp"))
    ny = 4
    grid = Mesh(mesh.devices.reshape(n_rep // ny, ny, n_fs, n_tp), ("z", "y", "fs", "tp"))
    split = P(("z", "y", "fs", "tp"), None)
    weight = P(None, "fs")
    grad = P(("z", "y", "tp"), "fs")
    return jax.shard_map(
        on_device,
        mesh=grid,
        in_specs=(split, split, weight, weight, weight),
        out_specs=(split, grad, grad, grad),
        check_vma=False,
    )
```

```python
import jax
import jax.numpy as jnp
from jax import lax
from jax.experimental import pallas as pl
from jax.experimental.pallas import tpu as pltpu
from jax.sharding import Mesh
from jax.sharding import PartitionSpec as P


F32 = jnp.float32
BF16 = jnp.bfloat16
NT = (((1,), (1,)), ((), ()))


def onward(value, axis, stride=1):
    n = lax.axis_size(axis)
    return lax.ppermute(value, (axis, "tp"), [(2 * i + c, 2 * ((i + stride * (1 - 2 * c)) % n) + c) for i in range(n) for c in range(2)])


def total(*values):
    return sum(v.astype(F32) for v in values)


def ring_gather(value):
    pieces = [value]
    for _ in range(1, 4):
        pieces.append(onward(pieces[-1], "fs"))
    return pieces


def ring_sum(parts, axis, stride=1):
    arrived = ()
    for k in range(len(parts) - 1, -1, -1):
        value = total(*parts[k], *arrived)
        value = value.astype(BF16) if k else value
        arrived = (onward(value, axis, stride),) if k else ()
    return value


def pair_place(owner, me, core, n):
    side = 1 - 2 * ((me + core) % 2)
    away = owner - me + n
    other = away % 2
    return other * (n // 2) + ((1 - 2 * core) * (away - other * side) + 4 * n) % n // 2


def pair_sum(parts, axis):
    n = parts[0].shape[0]
    perm = [(2 * i + c, 2 * ((i + 1 - 2 * ((i + c) % 2)) % n) + c) for i in range(n) for c in range(2)]
    value = total(*(p[n // 2 :] for p in parts)).astype(BF16)
    arrived = lax.ppermute(value, (axis, "tp"), perm)
    return direct_sum([tuple(p[k] for p in (*parts, arrived)) for k in range(n // 2)], axis, 2)


def direct_sum(parts, axis, stride):
    arrived = []
    for k in range(1, len(parts)):
        value = total(*parts[k]).astype(BF16)
        arrived.append(onward(value, axis, stride * k))
    return total(*parts[0], *arrived)


def resident(kernel, outs, operands, place, flops, scratch=()):
    nbytes = sum(v.size * v.dtype.itemsize for v in operands)
    return pl.pallas_call(
        kernel,
        in_specs=[pl.BlockSpec(memory_space=pltpu.SMEM)] + [pl.BlockSpec(memory_space=pltpu.VMEM)] * len(operands),
        out_specs=[pl.BlockSpec(memory_space=pltpu.VMEM)] * len(outs),
        out_shape=[pltpu.VMEM(shape, dtype) for shape, dtype in outs],
        scratch_shapes=scratch,
        compiler_params=pltpu.CompilerParams(vmem_limit_bytes=12 * 2**20),
        cost_estimate=pl.CostEstimate(flops=flops, bytes_accessed=nbytes, transcendentals=0),
    )(place, *(pltpu.with_memory_space_constraint(v, pltpu.VMEM) for v in operands))


def turned(pieces, place):
    width = pieces[0].shape[1]
    rows = sum(p.shape[0] for p in pieces)
    block = 256

    def kernel(_, *refs):
        def step(i, carry):
            at = pl.ds(pl.multiple_of(i * block, block), block)
            refs[-1][at, :] = jnp.concatenate([r[:, at] for r in refs[:-1]], axis=0).T
            return carry

        lax.fori_loop(0, width // block, step, 0)

    return resident(kernel, [((width, rows), BF16)], pieces, place, 16 * rows * width)[0]


def forward(pieces, gate_weight, up_weight, place):
    width, n = gate_weight.shape
    rows = sum(p.shape[0] for p in pieces)
    block = 256

    def kernel(_, *refs):
        gw, uw, hidden_ref, act_ref, slope_ref = refs[-5:]

        def step(i, carry):
            at = pl.ds(pl.multiple_of(i * block, block), block)
            tok = jnp.concatenate([r[...] for r in refs[:-5]], axis=0)
            gate_pre = jnp.dot(tok, gw[:, at], preferred_element_type=F32)
            up_pre = jnp.dot(tok, uw[:, at], preferred_element_type=F32)
            sig = jax.nn.sigmoid(gate_pre)
            act = gate_pre * sig
            hidden_ref[:, at] = (act * up_pre).astype(BF16)
            act_ref[:, at] = act
            slope_ref[:, at] = up_pre * (sig * (1.0 + gate_pre * (1.0 - sig)))
            return carry

        lax.fori_loop(0, n // block, step, 0)

    outs = [((rows, n), t) for t in (BF16, F32, F32)]
    return resident(kernel, outs, (*pieces, gate_weight, up_weight), place, 4 * rows * width * n)


def backward(pieces, down_weight_t, act, slope, place):
    width, n = down_weight_t.shape
    rows = sum(p.shape[0] for p in pieces)
    block = 256

    def kernel(_, *refs):
        dw, act_ref, slope_ref, gate_ref, up_ref = refs[-5:]

        def step(i, carry):
            at = pl.ds(pl.multiple_of(i * block, block), block)
            cot = jnp.concatenate([r[...] for r in refs[:-5]], axis=0)
            hid_grad = jnp.dot(cot, dw[:, at], preferred_element_type=F32)
            gate_ref[:, at] = (hid_grad * slope_ref[:, at]).astype(BF16)
            up_ref[:, at] = (hid_grad * act_ref[:, at]).astype(BF16)
            return carry

        lax.fori_loop(0, n // block, step, 0)

    outs = [((rows, n), BF16)] * 2
    return resident(kernel, outs, (*pieces, down_weight_t, act, slope), place, 2 * rows * width * n)


def weight_grad(near, far, rhs, place, sizes):
    width = near.shape[0]
    tokens, n = near.shape[1] + far.shape[1], rhs[0].shape[1]
    nz, ny = sizes
    rows = width // (nz * ny * 2)
    block = 2 * width // nz

    def kernel(place_ref, near_ref, far_ref, *refs):
        mine_ref, theirs_ref = refs[-2:]
        c, z, y = place_ref[0], place_ref[1], place_ref[2]
        way = 1 - 2 * c

        def step(i, carry):
            at = pl.ds(pl.multiple_of(i * block, block), block)
            lhs = jnp.concatenate([near_ref[at, :], far_ref[at, :]], axis=1)
            rhs = jnp.concatenate([r[...] for r in refs[:-2]], axis=0)
            out = jnp.dot(lhs, rhs, preferred_element_type=F32).reshape(2, ny, 2, rows, n)
            mine = jnp.where(c == 0, out[:, :, 0], out[:, :, 1]).astype(BF16)
            theirs = jnp.where(c == 0, out[:, :, 1], out[:, :, 0]).astype(BF16)
            for k in range(2):
                at_z = 2 * i + k
                mine_z, theirs_z = pair_place(at_z, z, c, nz), pair_place(at_z, z, 1 - c, nz)
                for j in range(ny):
                    mine_y = (way * (j - y) + 2 * ny) % ny
                    theirs_y = (ny - mine_y) % ny
                    mine_ref[mine_y, mine_z], theirs_ref[theirs_y, theirs_z] = mine[k, j], theirs[k, j]
            return carry

        lax.fori_loop(0, nz // 2, step, 0)

    shape = (ny, nz, rows, n)
    return resident(kernel, [(shape, BF16)] * 2, (near, far, *rhs), place, 2 * tokens * width * n)


def input_parts(gate_back, up_back, gate_weight, up_weight, place):
    n = gate_weight.shape[1]
    tokens = sum(v.shape[0] for v in gate_back)
    width = gate_weight.shape[0]
    block = 256
    rows = tokens // 4

    def kernel(_, *refs):
        (gw, uw), outs = refs[8:10], refs[10:]

        def step(i, carry):
            gb = jnp.concatenate([r[...] for r in refs[:4]], axis=0)
            ub = jnp.concatenate([r[...] for r in refs[4:8]], axis=0)
            at = pl.ds(pl.multiple_of(i * block, block), block)
            part = lax.dot_general(gb, gw[at, :], NT, preferred_element_type=F32)
            part = (part + lax.dot_general(ub, uw[at, :], NT, preferred_element_type=F32)).astype(BF16)
            for k in range(4):
                outs[(4 - k) % 4][:, at] = part[k * rows : (k + 1) * rows]
            return carry

        lax.fori_loop(0, width // block, step, 0)

    operands = (*gate_back, *up_back, gate_weight, up_weight)
    return resident(kernel, [((rows, width), BF16)] * 4, operands, place, 4 * tokens * width * n)


def with_partner(mine, theirs):
    return mine, lax.ppermute(theirs, "tp", [(0, 1), (1, 0)])


def by_place(parts):
    return [tuple(p[k] for p in parts) for k in range(parts[0].shape[0])]


def on_device(tokens, cotangent, gate_weight, up_weight, down_weight_t):
    sizes = lax.axis_size("z"), lax.axis_size("y")
    n_dev = sizes[0] * sizes[1] * lax.axis_size("fs") * lax.axis_size("tp")
    scale = float(tokens.shape[0] * n_dev) ** -0.5
    place = jnp.stack([lax.axis_index(a) for a in ("tp", "z", "y")]).astype(jnp.int32)
    tok = ring_gather(tokens)
    cot = ring_gather(cotangent)
    tok_near, tok_far = turned(tok[:3], place), turned(tok[3:], place)
    cot_near, cot_far = turned(cot[:3], place), turned(cot[3:], place)
    hidden, gate_back, up_back = [], [], []
    for k in range(4):
        hid, act, slope = forward(tok[k : k + 1], gate_weight, up_weight, place)
        gate, up = backward(cot[k : k + 1], down_weight_t, act, slope, place)
        hidden.append(hid)
        gate_back.append(gate)
        up_back.append(up)

    mine_g, theirs_g = weight_grad(tok_near, tok_far, gate_back, place, sizes)
    hidden[3], mine_g = lax.optimization_barrier((hidden[3], mine_g))
    mine_d, theirs_d = weight_grad(cot_near, cot_far, hidden, place, sizes)
    up_back[3], mine_d = lax.optimization_barrier((up_back[3], mine_d))
    mine_u, theirs_u = weight_grad(tok_near, tok_far, up_back, place, sizes)
    gate_back[3], up_back[3], mine_u = lax.optimization_barrier((gate_back[3], up_back[3], mine_u))
    parts = input_parts(gate_back, up_back, gate_weight, up_weight, place)

    plane_d = ring_sum(by_place(with_partner(mine_d, theirs_d)), "y").astype(BF16)
    plane_g = ring_sum(by_place(with_partner(mine_g, theirs_g)), "y").astype(BF16)
    plane_u = ring_sum(by_place(with_partner(mine_u, theirs_u)), "y").astype(BF16)
    input_grad = ring_sum([(p,) for p in parts], "fs").astype(BF16)
    both = jnp.concatenate([plane_g, plane_d], axis=2)
    both = pair_sum([both], "z") * scale
    up_grad = pair_sum([plane_u], "z") * scale
    n = gate_weight.shape[1]
    return input_grad, both[:, :n], up_grad, both[:, n:]


def solution(mesh):
    n_rep, n_fs, n_tp = (mesh.shape[a] for a in ("rep", "fs", "tp"))
    ny = 4
    grid = Mesh(mesh.devices.reshape(n_rep // ny, ny, n_fs, n_tp), ("z", "y", "fs", "tp"))
    split = P(("z", "y", "fs", "tp"), None)
    weight = P(None, "fs")
    grad = P(("z", "y", "tp"), "fs")
    return jax.shard_map(
        on_device,
        mesh=grid,
        in_specs=(split, split, weight, weight, weight),
        out_specs=(split, grad, grad, grad),
        check_vma=False,
    )
```

```python
import jax
import jax.numpy as jnp
from jax import lax
from jax.experimental import pallas as pl
from jax.experimental.pallas import tpu as pltpu
from jax.sharding import Mesh
from jax.sharding import PartitionSpec as P


F32 = jnp.float32
BF16 = jnp.bfloat16
NT = (((1,), (1,)), ((), ()))


def onward(value, axis, stride=1):
    n = lax.axis_size(axis)
    return lax.ppermute(value, (axis, "tp"), [(2 * i + c, 2 * ((i + stride * (1 - 2 * c)) % n) + c) for i in range(n) for c in range(2)])


def total(*values):
    return sum(v.astype(F32) for v in values)


def ring_gather(value):
    pieces = [value]
    for _ in range(1, 4):
        pieces.append(onward(pieces[-1], "fs"))
    return pieces


def ring_sum(parts, axis):
    arrived = ()
    for k in range(len(parts) - 1, -1, -1):
        value = total(*parts[k], *arrived)
        value = value.astype(BF16)
        arrived = (onward(value, axis),) if k else ()
    return value


def pair_place(owner, me, core, n):
    side = 1 - 2 * ((me + core) % 2)
    away = owner - me + n
    other = away % 2
    return other * (n // 2) + ((1 - 2 * core) * (away - other * side) + 4 * n) % n // 2


def pair_exchange(value, axis):
    n = lax.axis_size(axis)
    perm = [(2 * i + c, 2 * ((i + 1 - 2 * ((i + c) % 2)) % n) + c) for i in range(n) for c in range(2)]
    return lax.ppermute(value, (axis, "tp"), perm)


def y_then_pair(parts):
    plane = ring_sum(by_place(parts), "y")
    half = plane.shape[0] // 2
    arrived = pair_exchange(plane[half:], "z")
    return total(plane[:half], arrived).astype(BF16)


def pair_then_y(parts):
    half = parts[0].shape[1] // 2
    value = total(*(p[:, half:] for p in parts)).astype(BF16)
    arrived = pair_exchange(value, "z")
    return ring_sum(by_place([p[:, :half] for p in parts] + [arrived]), "y")


def direct_sum(parts, axis, stride):
    arrived = []
    for k in range(1, len(parts)):
        value = total(*parts[k]).astype(BF16)
        arrived.append(onward(value, axis, stride * k))
    return total(*parts[0], *arrived)


def resident(kernel, outs, operands, place, flops, scratch=()):
    nbytes = sum(v.size * v.dtype.itemsize for v in operands)
    return pl.pallas_call(
        kernel,
        in_specs=[pl.BlockSpec(memory_space=pltpu.SMEM)] + [pl.BlockSpec(memory_space=pltpu.VMEM)] * len(operands),
        out_specs=[pl.BlockSpec(memory_space=pltpu.VMEM)] * len(outs),
        out_shape=[pltpu.VMEM(shape, dtype) for shape, dtype in outs],
        scratch_shapes=scratch,
        compiler_params=pltpu.CompilerParams(vmem_limit_bytes=12 * 2**20),
        cost_estimate=pl.CostEstimate(flops=flops, bytes_accessed=nbytes, transcendentals=0),
    )(place, *(pltpu.with_memory_space_constraint(v, pltpu.VMEM) for v in operands))


def turned(pieces, place):
    width = pieces[0].shape[1]
    rows = sum(p.shape[0] for p in pieces)
    block = 256

    def kernel(_, *refs):
        def step(i, carry):
            at = pl.ds(pl.multiple_of(i * block, block), block)
            refs[-1][at, :] = jnp.concatenate([r[:, at] for r in refs[:-1]], axis=0).T
            return carry

        lax.fori_loop(0, width // block, step, 0)

    return resident(kernel, [((width, rows), BF16)], pieces, place, 16 * rows * width)[0]


def forward(pieces, gate_weight, up_weight, place):
    width, n = gate_weight.shape
    rows = sum(p.shape[0] for p in pieces)
    block = 256

    def kernel(_, *refs):
        gw, uw, hidden_ref, act_ref, slope_ref = refs[-5:]

        def step(i, carry):
            at = pl.ds(pl.multiple_of(i * block, block), block)
            tok = jnp.concatenate([r[...] for r in refs[:-5]], axis=0)
            gate_pre = jnp.dot(tok, gw[:, at], preferred_element_type=F32)
            up_pre = jnp.dot(tok, uw[:, at], preferred_element_type=F32)
            sig = jax.nn.sigmoid(gate_pre)
            act = gate_pre * sig
            hidden_ref[:, at] = (act * up_pre).astype(BF16)
            act_ref[:, at] = act
            slope_ref[:, at] = up_pre * (sig * (1.0 + gate_pre * (1.0 - sig)))
            return carry

        lax.fori_loop(0, n // block, step, 0)

    outs = [((rows, n), t) for t in (BF16, F32, F32)]
    return resident(kernel, outs, (*pieces, gate_weight, up_weight), place, 4 * rows * width * n)


def backward(pieces, down_weight_t, act, slope, place):
    width, n = down_weight_t.shape
    rows = sum(p.shape[0] for p in pieces)
    block = 256

    def kernel(_, *refs):
        dw, act_ref, slope_ref, gate_ref, up_ref = refs[-5:]

        def step(i, carry):
            at = pl.ds(pl.multiple_of(i * block, block), block)
            cot = jnp.concatenate([r[...] for r in refs[:-5]], axis=0)
            hid_grad = jnp.dot(cot, dw[:, at], preferred_element_type=F32)
            gate_ref[:, at] = (hid_grad * slope_ref[:, at]).astype(BF16)
            up_ref[:, at] = (hid_grad * act_ref[:, at]).astype(BF16)
            return carry

        lax.fori_loop(0, n // block, step, 0)

    outs = [((rows, n), BF16)] * 2
    return resident(kernel, outs, (*pieces, down_weight_t, act, slope), place, 2 * rows * width * n)


def weight_grad(near, far, rhs, place, sizes):
    width = near.shape[0]
    tokens, n = near.shape[1] + far.shape[1], rhs[0].shape[1]
    nz, ny = sizes
    rows = width // (nz * ny * 2)
    block = 2 * width // nz

    def kernel(place_ref, near_ref, far_ref, *refs):
        mine_ref, theirs_ref = refs[-2:]
        c, z, y = place_ref[0], place_ref[1], place_ref[2]
        way = 1 - 2 * c

        def step(i, carry):
            at = pl.ds(pl.multiple_of(i * block, block), block)
            lhs = jnp.concatenate([near_ref[at, :], far_ref[at, :]], axis=1)
            rhs = jnp.concatenate([r[...] for r in refs[:-2]], axis=0)
            out = jnp.dot(lhs, rhs, preferred_element_type=F32).reshape(2, ny, 2, rows, n)
            mine = jnp.where(c == 0, out[:, :, 0], out[:, :, 1]).astype(BF16)
            theirs = jnp.where(c == 0, out[:, :, 1], out[:, :, 0]).astype(BF16)
            for k in range(2):
                at_z = 2 * i + k
                mine_z, theirs_z = pair_place(at_z, z, c, nz), pair_place(at_z, z, 1 - c, nz)
                for j in range(ny):
                    mine_y = (way * (j - y) + 2 * ny) % ny
                    theirs_y = (ny - mine_y) % ny
                    mine_ref[mine_y, mine_z], theirs_ref[theirs_y, theirs_z] = mine[k, j], theirs[k, j]
            return carry

        lax.fori_loop(0, nz // 2, step, 0)

    shape = (ny, nz, rows, n)
    return resident(kernel, [(shape, BF16)] * 2, (near, far, *rhs), place, 2 * tokens * width * n)


def input_parts(gate_back, up_back, gate_weight, up_weight, place):
    n = gate_weight.shape[1]
    tokens = sum(v.shape[0] for v in gate_back)
    width = gate_weight.shape[0]
    block = 256
    rows = tokens // 4

    def kernel(_, *refs):
        (gw, uw), outs = refs[8:10], refs[10:]

        def step(i, carry):
            gb = jnp.concatenate([r[...] for r in refs[:4]], axis=0)
            ub = jnp.concatenate([r[...] for r in refs[4:8]], axis=0)
            at = pl.ds(pl.multiple_of(i * block, block), block)
            part = lax.dot_general(gb, gw[at, :], NT, preferred_element_type=F32)
            part = (part + lax.dot_general(ub, uw[at, :], NT, preferred_element_type=F32)).astype(BF16)
            for k in range(4):
                outs[(4 - k) % 4][:, at] = part[k * rows : (k + 1) * rows]
            return carry

        lax.fori_loop(0, width // block, step, 0)

    operands = (*gate_back, *up_back, gate_weight, up_weight)
    return resident(kernel, [((rows, width), BF16)] * 4, operands, place, 4 * tokens * width * n)


def with_partner(mine, theirs):
    return mine, lax.ppermute(theirs, "tp", [(0, 1), (1, 0)])


def by_place(parts):
    return [tuple(p[k] for p in parts) for k in range(parts[0].shape[0])]


def on_device(tokens, cotangent, gate_weight, up_weight, down_weight_t):
    sizes = lax.axis_size("z"), lax.axis_size("y")
    n_dev = sizes[0] * sizes[1] * lax.axis_size("fs") * lax.axis_size("tp")
    scale = float(tokens.shape[0] * n_dev) ** -0.5
    place = jnp.stack([lax.axis_index(a) for a in ("tp", "z", "y")]).astype(jnp.int32)
    tok = ring_gather(tokens)
    cot = ring_gather(cotangent)
    tok_near, tok_far = turned(tok[:3], place), turned(tok[3:], place)
    cot_near, cot_far = turned(cot[:3], place), turned(cot[3:], place)
    hidden, gate_back, up_back = [], [], []
    for k in range(4):
        hid, act, slope = forward(tok[k : k + 1], gate_weight, up_weight, place)
        gate, up = backward(cot[k : k + 1], down_weight_t, act, slope, place)
        hidden.append(hid)
        gate_back.append(gate)
        up_back.append(up)

    mine_g, theirs_g = weight_grad(tok_near, tok_far, gate_back, place, sizes)
    hidden[3], mine_g = lax.optimization_barrier((hidden[3], mine_g))
    mine_d, theirs_d = weight_grad(cot_near, cot_far, hidden, place, sizes)
    up_back[3], mine_d = lax.optimization_barrier((up_back[3], mine_d))
    mine_u, theirs_u = weight_grad(tok_near, tok_far, up_back, place, sizes)
    gate_back[3], up_back[3], mine_u = lax.optimization_barrier((gate_back[3], up_back[3], mine_u))
    parts = input_parts(gate_back, up_back, gate_weight, up_weight, place)

    half_g = y_then_pair(with_partner(mine_g, theirs_g))
    half_d = pair_then_y(with_partner(mine_d, theirs_d))
    half_u = pair_then_y(with_partner(mine_u, theirs_u))
    input_grad = ring_sum([(p,) for p in parts], "fs")
    both = jnp.concatenate([half_g, half_d], axis=2)
    both = direct_sum(by_place([both]), "z", 2) * scale
    up_grad = direct_sum(by_place([half_u]), "z", 2) * scale
    n = gate_weight.shape[1]
    return input_grad, both[:, :n], up_grad, both[:, n:]


def solution(mesh):
    n_rep, n_fs, n_tp = (mesh.shape[a] for a in ("rep", "fs", "tp"))
    ny = 4
    grid = Mesh(mesh.devices.reshape(n_rep // ny, ny, n_fs, n_tp), ("z", "y", "fs", "tp"))
    split = P(("z", "y", "fs", "tp"), None)
    weight = P(None, "fs")
    grad = P(("z", "y", "tp"), "fs")
    return jax.shard_map(
        on_device,
        mesh=grid,
        in_specs=(split, split, weight, weight, weight),
        out_specs=(split, grad, grad, grad),
        check_vma=False,
    )
```

```python
import jax
import jax.numpy as jnp
from jax import lax
from jax.experimental import pallas as pl
from jax.experimental.pallas import tpu as pltpu
from jax.sharding import Mesh
from jax.sharding import PartitionSpec as P


F32 = jnp.float32
BF16 = jnp.bfloat16
NT = (((1,), (1,)), ((), ()))


def onward(value, axis, stride=1):
    n = lax.axis_size(axis)
    return lax.ppermute(value, (axis, "tp"), [(2 * i + c, 2 * ((i + stride * (1 - 2 * c)) % n) + c) for i in range(n) for c in range(2)])


def total(*values):
    return sum(v.astype(F32) for v in values)


def ring_gather(value):
    pieces = [value]
    for _ in range(1, 4):
        pieces.append(onward(pieces[-1], "fs"))
    return pieces


def ring_sum(parts, axis):
    arrived = ()
    for k in range(len(parts) - 1, -1, -1):
        value = total(*parts[k], *arrived)
        value = value.astype(BF16)
        arrived = (onward(value, axis),) if k else ()
    return value


def pair_place(owner, me, core, n):
    side = 1 - 2 * ((me + core) % 2)
    away = owner - me + n
    other = away % 2
    return other * (n // 2) + ((1 - 2 * core) * (away - other * side) + 4 * n) % n // 2


def pair_exchange(value, axis):
    n = lax.axis_size(axis)
    perm = [(2 * i + c, 2 * ((i + 1 - 2 * ((i + c) % 2)) % n) + c) for i in range(n) for c in range(2)]
    return lax.ppermute(value, (axis, "tp"), perm)


def pair_then_y(parts):
    half = parts[0].shape[1] // 2
    value = total(*(p[:, half:] for p in parts)).astype(BF16)
    arrived = pair_exchange(value, "z")
    return direct_sum(by_place([p[:, :half] for p in parts] + [arrived]), "y", 1, BF16)


def direct_sum(parts, axis, stride, dtype):
    arrived = []
    for k in range(1, len(parts)):
        value = total(*parts[k]).astype(BF16)
        arrived.append(onward(value, axis, stride * k))
    return total(*parts[0], *arrived).astype(dtype)


def resident(kernel, outs, operands, place, flops, scratch=()):
    nbytes = sum(v.size * v.dtype.itemsize for v in operands)
    return pl.pallas_call(
        kernel,
        in_specs=[pl.BlockSpec(memory_space=pltpu.SMEM)] + [pl.BlockSpec(memory_space=pltpu.VMEM)] * len(operands),
        out_specs=[pl.BlockSpec(memory_space=pltpu.VMEM)] * len(outs),
        out_shape=[pltpu.VMEM(shape, dtype) for shape, dtype in outs],
        scratch_shapes=scratch,
        compiler_params=pltpu.CompilerParams(vmem_limit_bytes=12 * 2**20),
        cost_estimate=pl.CostEstimate(flops=flops, bytes_accessed=nbytes, transcendentals=0),
    )(place, *(pltpu.with_memory_space_constraint(v, pltpu.VMEM) for v in operands))


def turned(pieces, place):
    width = pieces[0].shape[1]
    rows = sum(p.shape[0] for p in pieces)
    block = 256

    def kernel(_, *refs):
        def step(i, carry):
            at = pl.ds(pl.multiple_of(i * block, block), block)
            refs[-1][at, :] = jnp.concatenate([r[:, at] for r in refs[:-1]], axis=0).T
            return carry

        lax.fori_loop(0, width // block, step, 0)

    return resident(kernel, [((width, rows), BF16)], pieces, place, 16 * rows * width)[0]


def forward(pieces, gate_weight, up_weight, place):
    width, n = gate_weight.shape
    rows = sum(p.shape[0] for p in pieces)
    block = 256

    def kernel(_, *refs):
        gw, uw, hidden_ref, act_ref, slope_ref = refs[-5:]

        def step(i, carry):
            at = pl.ds(pl.multiple_of(i * block, block), block)
            tok = jnp.concatenate([r[...] for r in refs[:-5]], axis=0)
            gate_pre = jnp.dot(tok, gw[:, at], preferred_element_type=F32)
            up_pre = jnp.dot(tok, uw[:, at], preferred_element_type=F32)
            sig = jax.nn.sigmoid(gate_pre)
            act = gate_pre * sig
            hidden_ref[:, at] = (act * up_pre).astype(BF16)
            act_ref[:, at] = act
            slope_ref[:, at] = up_pre * (sig * (1.0 + gate_pre * (1.0 - sig)))
            return carry

        lax.fori_loop(0, n // block, step, 0)

    outs = [((rows, n), t) for t in (BF16, F32, F32)]
    return resident(kernel, outs, (*pieces, gate_weight, up_weight), place, 4 * rows * width * n)


def backward(pieces, down_weight_t, act, slope, place):
    width, n = down_weight_t.shape
    rows = sum(p.shape[0] for p in pieces)
    block = 256

    def kernel(_, *refs):
        dw, act_ref, slope_ref, gate_ref, up_ref = refs[-5:]

        def step(i, carry):
            at = pl.ds(pl.multiple_of(i * block, block), block)
            cot = jnp.concatenate([r[...] for r in refs[:-5]], axis=0)
            hid_grad = jnp.dot(cot, dw[:, at], preferred_element_type=F32)
            gate_ref[:, at] = (hid_grad * slope_ref[:, at]).astype(BF16)
            up_ref[:, at] = (hid_grad * act_ref[:, at]).astype(BF16)
            return carry

        lax.fori_loop(0, n // block, step, 0)

    outs = [((rows, n), BF16)] * 2
    return resident(kernel, outs, (*pieces, down_weight_t, act, slope), place, 2 * rows * width * n)


def weight_grad(near, far, rhs, place, sizes):
    width = near.shape[0]
    tokens, n = near.shape[1] + far.shape[1], rhs[0].shape[1]
    nz, ny = sizes
    rows = width // (nz * ny * 2)
    block = 2 * width // nz

    def kernel(place_ref, near_ref, far_ref, *refs):
        mine_ref, theirs_ref = refs[-2:]
        c, z, y = place_ref[0], place_ref[1], place_ref[2]
        way = 1 - 2 * c

        def step(i, carry):
            at = pl.ds(pl.multiple_of(i * block, block), block)
            lhs = jnp.concatenate([near_ref[at, :], far_ref[at, :]], axis=1)
            rhs = jnp.concatenate([r[...] for r in refs[:-2]], axis=0)
            out = jnp.dot(lhs, rhs, preferred_element_type=F32).reshape(2, ny, 2, rows, n)
            mine = jnp.where(c == 0, out[:, :, 0], out[:, :, 1]).astype(BF16)
            theirs = jnp.where(c == 0, out[:, :, 1], out[:, :, 0]).astype(BF16)
            for k in range(2):
                at_z = 2 * i + k
                mine_z, theirs_z = pair_place(at_z, z, c, nz), pair_place(at_z, z, 1 - c, nz)
                for j in range(ny):
                    mine_y = (way * (j - y) + 2 * ny) % ny
                    theirs_y = (ny - mine_y) % ny
                    mine_ref[mine_y, mine_z], theirs_ref[theirs_y, theirs_z] = mine[k, j], theirs[k, j]
            return carry

        lax.fori_loop(0, nz // 2, step, 0)

    shape = (ny, nz, rows, n)
    return resident(kernel, [(shape, BF16)] * 2, (near, far, *rhs), place, 2 * tokens * width * n)


def input_parts(gate_back, up_back, gate_weight, up_weight, place):
    n = gate_weight.shape[1]
    tokens = sum(v.shape[0] for v in gate_back)
    width = gate_weight.shape[0]
    block = 256
    rows = tokens // 4

    def kernel(_, *refs):
        (gw, uw), outs = refs[8:10], refs[10:]

        def step(i, carry):
            gb = jnp.concatenate([r[...] for r in refs[:4]], axis=0)
            ub = jnp.concatenate([r[...] for r in refs[4:8]], axis=0)
            at = pl.ds(pl.multiple_of(i * block, block), block)
            part = lax.dot_general(gb, gw[at, :], NT, preferred_element_type=F32)
            part = (part + lax.dot_general(ub, uw[at, :], NT, preferred_element_type=F32)).astype(BF16)
            for k in range(4):
                outs[(4 - k) % 4][:, at] = part[k * rows : (k + 1) * rows]
            return carry

        lax.fori_loop(0, width // block, step, 0)

    operands = (*gate_back, *up_back, gate_weight, up_weight)
    return resident(kernel, [((rows, width), BF16)] * 4, operands, place, 4 * tokens * width * n)


def with_partner(mine, theirs):
    return mine, lax.ppermute(theirs, "tp", [(0, 1), (1, 0)])


def by_place(parts):
    return [tuple(p[k] for p in parts) for k in range(parts[0].shape[0])]


def on_device(tokens, cotangent, gate_weight, up_weight, down_weight_t):
    sizes = lax.axis_size("z"), lax.axis_size("y")
    n_dev = sizes[0] * sizes[1] * lax.axis_size("fs") * lax.axis_size("tp")
    scale = float(tokens.shape[0] * n_dev) ** -0.5
    place = jnp.stack([lax.axis_index(a) for a in ("tp", "z", "y")]).astype(jnp.int32)
    tok = ring_gather(tokens)
    cot = ring_gather(cotangent)
    tok_near, tok_far = turned(tok[:3], place), turned(tok[3:], place)
    cot_near, cot_far = turned(cot[:3], place), turned(cot[3:], place)
    hidden, gate_back, up_back = [], [], []
    for k in range(4):
        hid, act, slope = forward(tok[k : k + 1], gate_weight, up_weight, place)
        gate, up = backward(cot[k : k + 1], down_weight_t, act, slope, place)
        hidden.append(hid)
        gate_back.append(gate)
        up_back.append(up)

    mine_g, theirs_g = weight_grad(tok_near, tok_far, gate_back, place, sizes)
    hidden[3], mine_g = lax.optimization_barrier((hidden[3], mine_g))
    mine_d, theirs_d = weight_grad(cot_near, cot_far, hidden, place, sizes)
    up_back[3], mine_d = lax.optimization_barrier((up_back[3], mine_d))
    mine_u, theirs_u = weight_grad(tok_near, tok_far, up_back, place, sizes)
    gate_back[3], up_back[3], mine_u = lax.optimization_barrier((gate_back[3], up_back[3], mine_u))
    parts = input_parts(gate_back, up_back, gate_weight, up_weight, place)

    half_g = pair_then_y(with_partner(mine_g, theirs_g))
    half_d = pair_then_y(with_partner(mine_d, theirs_d))
    half_u = pair_then_y(with_partner(mine_u, theirs_u))
    input_grad = ring_sum([(p,) for p in parts], "fs")
    both = jnp.concatenate([half_g, half_d], axis=2)
    both = direct_sum(by_place([both]), "z", 2, F32) * scale
    up_grad = direct_sum(by_place([half_u]), "z", 2, F32) * scale
    n = gate_weight.shape[1]
    return input_grad, both[:, :n], up_grad, both[:, n:]


def solution(mesh):
    n_rep, n_fs, n_tp = (mesh.shape[a] for a in ("rep", "fs", "tp"))
    ny = 4
    grid = Mesh(mesh.devices.reshape(n_rep // ny, ny, n_fs, n_tp), ("z", "y", "fs", "tp"))
    split = P(("z", "y", "fs", "tp"), None)
    weight = P(None, "fs")
    grad = P(("z", "y", "tp"), "fs")
    return jax.shard_map(
        on_device,
        mesh=grid,
        in_specs=(split, split, weight, weight, weight),
        out_specs=(split, grad, grad, grad),
        check_vma=False,
    )
```

```python
import jax
import jax.numpy as jnp
from jax import lax
from jax.experimental import pallas as pl
from jax.experimental.pallas import tpu as pltpu
from jax.sharding import Mesh
from jax.sharding import PartitionSpec as P


F32 = jnp.float32
BF16 = jnp.bfloat16
NT = (((1,), (1,)), ((), ()))


def onward(value, axis, stride=1):
    n = lax.axis_size(axis)
    return lax.ppermute(value, (axis, "tp"), [(2 * i + c, 2 * ((i + stride * (1 - 2 * c)) % n) + c) for i in range(n) for c in range(2)])


def total(*values):
    return sum(v.astype(F32) for v in values)


def ring_gather(value):
    pieces = [value]
    for _ in range(1, 4):
        pieces.append(onward(pieces[-1], "fs"))
    return pieces


def ring_sum(parts, axis):
    arrived = ()
    for k in range(len(parts) - 1, -1, -1):
        value = total(*parts[k], *arrived)
        value = value.astype(BF16)
        arrived = (onward(value, axis),) if k else ()
    return value


def pair_place(owner, me, core, n):
    side = 1 - 2 * ((me + core) % 2)
    away = owner - me + n
    other = away % 2
    return other * (n // 2) + ((1 - 2 * core) * (away - other * side) + 4 * n) % n // 2


def pair_exchange(value, axis):
    n = lax.axis_size(axis)
    perm = [(2 * i + c, 2 * ((i + 1 - 2 * ((i + c) % 2)) % n) + c) for i in range(n) for c in range(2)]
    return lax.ppermute(value, (axis, "tp"), perm)


def pair_then_y(parts):
    half = parts[0].shape[1] // 2
    value = total(*(p[:, half:] for p in parts)).astype(BF16)
    arrived = pair_exchange(value, "z")
    return direct_sum(by_place([p[:, :half] for p in parts] + [arrived]), "y", 1, BF16)


def y_then_pair(parts):
    plane = direct_sum(by_place(parts), "y", 1, BF16)
    half = plane.shape[0] // 2
    arrived = pair_exchange(plane[half:], "z")
    return total(plane[:half], arrived).astype(BF16)


def direct_sum(parts, axis, stride, dtype):
    arrived = []
    for k in range(1, len(parts)):
        value = total(*parts[k]).astype(BF16)
        arrived.append(onward(value, axis, stride * k))
    return total(*parts[0], *arrived).astype(dtype)


def resident(kernel, outs, operands, place, flops, scratch=()):
    nbytes = sum(v.size * v.dtype.itemsize for v in operands)
    return pl.pallas_call(
        kernel,
        in_specs=[pl.BlockSpec(memory_space=pltpu.SMEM)] + [pl.BlockSpec(memory_space=pltpu.VMEM)] * len(operands),
        out_specs=[pl.BlockSpec(memory_space=pltpu.VMEM)] * len(outs),
        out_shape=[pltpu.VMEM(shape, dtype) for shape, dtype in outs],
        scratch_shapes=scratch,
        compiler_params=pltpu.CompilerParams(vmem_limit_bytes=12 * 2**20),
        cost_estimate=pl.CostEstimate(flops=flops, bytes_accessed=nbytes, transcendentals=0),
    )(place, *(pltpu.with_memory_space_constraint(v, pltpu.VMEM) for v in operands))


def turned(pieces, place):
    width = pieces[0].shape[1]
    rows = sum(p.shape[0] for p in pieces)
    block = 256

    def kernel(_, *refs):
        def step(i, carry):
            at = pl.ds(pl.multiple_of(i * block, block), block)
            refs[-1][at, :] = jnp.concatenate([r[:, at] for r in refs[:-1]], axis=0).T
            return carry

        lax.fori_loop(0, width // block, step, 0)

    return resident(kernel, [((width, rows), BF16)], pieces, place, 16 * rows * width)[0]


def forward(pieces, gate_weight, up_weight, place):
    width, n = gate_weight.shape
    rows = sum(p.shape[0] for p in pieces)
    block = 256

    def kernel(_, *refs):
        gw, uw, hidden_ref, act_ref, slope_ref = refs[-5:]

        def step(i, carry):
            at = pl.ds(pl.multiple_of(i * block, block), block)
            tok = jnp.concatenate([r[...] for r in refs[:-5]], axis=0)
            gate_pre = jnp.dot(tok, gw[:, at], preferred_element_type=F32)
            up_pre = jnp.dot(tok, uw[:, at], preferred_element_type=F32)
            sig = jax.nn.sigmoid(gate_pre)
            act = gate_pre * sig
            hidden_ref[:, at] = (act * up_pre).astype(BF16)
            act_ref[:, at] = act
            slope_ref[:, at] = up_pre * (sig * (1.0 + gate_pre * (1.0 - sig)))
            return carry

        lax.fori_loop(0, n // block, step, 0)

    outs = [((rows, n), t) for t in (BF16, F32, F32)]
    return resident(kernel, outs, (*pieces, gate_weight, up_weight), place, 4 * rows * width * n)


def backward(pieces, down_weight_t, act, slope, place):
    width, n = down_weight_t.shape
    rows = sum(p.shape[0] for p in pieces)
    block = 256

    def kernel(_, *refs):
        dw, act_ref, slope_ref, gate_ref, up_ref = refs[-5:]

        def step(i, carry):
            at = pl.ds(pl.multiple_of(i * block, block), block)
            cot = jnp.concatenate([r[...] for r in refs[:-5]], axis=0)
            hid_grad = jnp.dot(cot, dw[:, at], preferred_element_type=F32)
            gate_ref[:, at] = (hid_grad * slope_ref[:, at]).astype(BF16)
            up_ref[:, at] = (hid_grad * act_ref[:, at]).astype(BF16)
            return carry

        lax.fori_loop(0, n // block, step, 0)

    outs = [((rows, n), BF16)] * 2
    return resident(kernel, outs, (*pieces, down_weight_t, act, slope), place, 2 * rows * width * n)


def weight_grad(near, far, rhs, place, sizes):
    width = near.shape[0]
    tokens, n = near.shape[1] + far.shape[1], rhs[0].shape[1]
    nz, ny = sizes
    rows = width // (nz * ny * 2)
    block = 2 * width // nz

    def kernel(place_ref, near_ref, far_ref, *refs):
        mine_ref, theirs_ref = refs[-2:]
        c, z, y = place_ref[0], place_ref[1], place_ref[2]
        way = 1 - 2 * c

        def step(i, carry):
            at = pl.ds(pl.multiple_of(i * block, block), block)
            lhs = jnp.concatenate([near_ref[at, :], far_ref[at, :]], axis=1)
            rhs = jnp.concatenate([r[...] for r in refs[:-2]], axis=0)
            out = jnp.dot(lhs, rhs, preferred_element_type=F32).reshape(2, ny, 2, rows, n)
            first, second = out[:, :, 0].astype(BF16), out[:, :, 1].astype(BF16)
            mine, theirs = jnp.where(c == 0, first, second), jnp.where(c == 0, second, first)
            for k in range(2):
                at_z = 2 * i + k
                mine_z, theirs_z = pair_place(at_z, z, c, nz), pair_place(at_z, z, 1 - c, nz)
                for j in range(ny):
                    mine_y = (way * (j - y) + 2 * ny) % ny
                    theirs_y = (ny - mine_y) % ny
                    mine_ref[mine_y, mine_z], theirs_ref[theirs_y, theirs_z] = mine[k, j], theirs[k, j]
            return carry

        lax.fori_loop(0, nz // 2, step, 0)

    shape = (ny, nz, rows, n)
    return resident(kernel, [(shape, BF16)] * 2, (near, far, *rhs), place, 2 * tokens * width * n)


def input_parts(gate_back, up_back, gate_weight, up_weight, place):
    n = gate_weight.shape[1]
    tokens = sum(v.shape[0] for v in gate_back)
    width = gate_weight.shape[0]
    block = 256
    rows = tokens // 4

    def kernel(_, *refs):
        (gw, uw), outs = refs[8:10], refs[10:]

        def step(i, carry):
            at = pl.ds(pl.multiple_of(i * block, block), block)
            back = [jnp.concatenate([r[...] for r in refs[j : j + 4]], axis=0) for j in (0, 4)]
            weights = jnp.concatenate([gw[at, :], uw[at, :]], axis=1)
            part = lax.dot_general(jnp.concatenate(back, axis=1), weights, NT, preferred_element_type=F32)
            part = part.astype(BF16)
            for k in range(4):
                outs[(4 - k) % 4][:, at] = part[k * rows : (k + 1) * rows]
            return carry

        lax.fori_loop(0, width // block, step, 0)

    operands = (*gate_back, *up_back, gate_weight, up_weight)
    return resident(kernel, [((rows, width), BF16)] * 4, operands, place, 4 * tokens * width * n)


def with_partner(mine, theirs):
    return mine, lax.ppermute(theirs, "tp", [(0, 1), (1, 0)])


def by_place(parts):
    return [tuple(p[k] for p in parts) for k in range(parts[0].shape[0])]


def on_device(tokens, cotangent, gate_weight, up_weight, down_weight_t):
    sizes = lax.axis_size("z"), lax.axis_size("y")
    n_dev = sizes[0] * sizes[1] * lax.axis_size("fs") * lax.axis_size("tp")
    scale = float(tokens.shape[0] * n_dev) ** -0.5
    place = jnp.stack([lax.axis_index(a) for a in ("tp", "z", "y")]).astype(jnp.int32)
    tok = ring_gather(tokens)
    cot = ring_gather(cotangent)
    tok_near, tok_far = turned(tok[:3], place), turned(tok[3:], place)
    cot_near, cot_far = turned(cot[:3], place), turned(cot[3:], place)
    hidden, gate_back, up_back = [], [], []
    for k in range(4):
        hid, act, slope = forward(tok[k : k + 1], gate_weight, up_weight, place)
        gate, up = backward(cot[k : k + 1], down_weight_t, act, slope, place)
        hidden.append(hid)
        gate_back.append(gate)
        up_back.append(up)

    mine_g, theirs_g = weight_grad(tok_near, tok_far, gate_back, place, sizes)
    hidden[3], mine_g = lax.optimization_barrier((hidden[3], mine_g))
    mine_d, theirs_d = weight_grad(cot_near, cot_far, hidden, place, sizes)
    up_back[3], mine_d = lax.optimization_barrier((up_back[3], mine_d))
    mine_u, theirs_u = weight_grad(tok_near, tok_far, up_back, place, sizes)
    gate_back[3], up_back[3], mine_u = lax.optimization_barrier((gate_back[3], up_back[3], mine_u))
    parts = input_parts(gate_back, up_back, gate_weight, up_weight, place)

    half_g = y_then_pair(with_partner(mine_g, theirs_g))
    half_d = pair_then_y(with_partner(mine_d, theirs_d))
    half_u = pair_then_y(with_partner(mine_u, theirs_u))
    input_grad = ring_sum([(p,) for p in parts], "fs")
    both = jnp.concatenate([half_g, half_d], axis=2)
    both = direct_sum(by_place([both]), "z", 2, F32) * scale
    up_grad = direct_sum(by_place([half_u]), "z", 2, F32) * scale
    n = gate_weight.shape[1]
    return input_grad, both[:, :n], up_grad, both[:, n:]


def solution(mesh):
    n_rep, n_fs, n_tp = (mesh.shape[a] for a in ("rep", "fs", "tp"))
    ny = 4
    grid = Mesh(mesh.devices.reshape(n_rep // ny, ny, n_fs, n_tp), ("z", "y", "fs", "tp"))
    split = P(("z", "y", "fs", "tp"), None)
    weight = P(None, "fs")
    grad = P(("z", "y", "tp"), "fs")
    return jax.shard_map(
        on_device,
        mesh=grid,
        in_specs=(split, split, weight, weight, weight),
        out_specs=(split, grad, grad, grad),
        check_vma=False,
    )
```
